512 devices in a mesh: sp: 64 (over z, y), tp: 8 (over x, core).
Axes of the slice: x: 4, y: 4, z: 16, core: 2. Of those that a mesh axis runs over, the one named last changes fastest.
Arguments:
- queries: bfloat16 [12288, 1024], P('sp', 'tp'), may hold values from -6 to 6
- keys: bfloat16 [12288, 512], P('sp', 'tp'), may hold values from -6 to 6
- values: bfloat16 [12288, 512], P('sp', 'tp'), may hold values from -6 to 6
- query_gain: float32 [16, 64], P('tp'), may hold values from 1.4 to 7.5
- key_gain: float32 [8, 64], P('tp'), may hold values from 1.4 to 7.5
- out_weight: bfloat16 [1024, 2048], P('tp'), may hold values from -0.375 to 0.375
- residual: bfloat16 [12288, 2048], P('sp'), may hold values from -170 to 170
- norm_gain: float32 [2048], replicated, may hold values from 0.1 to 1.9
- gate_weight: bfloat16 [2048, 5632], P('sp', 'tp'), may hold values from -0.125 to 0.125
- up_weight: bfloat16 [2048, 5632], P('sp', 'tp'), may hold values from -0.125 to 0.125
- down_weight: bfloat16 [5632, 2048], P('tp', 'sp'), may hold values from -0.15625 to 0.15625
Outputs:
- mixed: bfloat16 [12288, 2048], P('sp')
The draws below stay inside these ranges and needn't reach their ends.
All inputs are finite; a program needn't handle non-finite values.
Results may differ from the reference program's by a relative error of at most 0.017.
Values may be sent and summed in bfloat16 or wider, within the bound.
A program may use at most 64 MiB of HBM per device.

```python
import math
import jax
import jax.numpy as jnp
from jax import lax

D = 2048
FF = 5632
HEADS = 16
KV_HEADS = 8
HEAD_SIZE = 64
GRID_W = 64
SEQ = 12288
N_TP = 8


def drawn_keys(key):
    base_keys = jnp.clip(jax.random.normal(jax.random.fold_in(key, 11), (SEQ, KV_HEADS * HEAD_SIZE), jnp.float32), -6.0, 6.0)
    return base_keys


def draw_keys(key, part):
    base_keys = drawn_keys(key)
    return base_keys.astype(jnp.bfloat16)


def draw_queries(key, part):
    fresh = jnp.clip(jax.random.normal(jax.random.fold_in(key, 12), (SEQ, HEADS * HEAD_SIZE), jnp.float32), -6.0, 6.0)
    return fresh.astype(jnp.bfloat16)


def draw_values(key, part):
    column_sign = jnp.where(jax.random.uniform(jax.random.fold_in(key, 51), (1, KV_HEADS * HEAD_SIZE), jnp.float32) < 0.5, -1.0, 1.0)
    noise = jax.random.normal(jax.random.fold_in(key, 52), (SEQ, KV_HEADS * HEAD_SIZE), jnp.float32)
    return jnp.clip(2.0 * column_sign + noise, -6.0, 6.0).astype(jnp.bfloat16)


def gain_levels(key, count, salt):
    lower, upper = (1.7, 2.0)
    level = jnp.exp(jax.random.uniform(jax.random.fold_in(key, salt), (count, 1), jnp.float32, jnp.log(lower), jnp.log(upper)))
    rough = jax.random.uniform(jax.random.fold_in(key, salt + 1), (count, HEAD_SIZE), jnp.float32, 0.85, 1.15)
    return level * rough


def draw_query_gain(key, part):
    return gain_levels(key, HEADS, 31)


def draw_key_gain(key, part):
    return gain_levels(key, KV_HEADS, 41)


def draw_residual(key, part):
    base = jnp.clip(jax.random.normal(jax.random.fold_in(key, 21), (SEQ, D), jnp.float32), -6.0, 6.0)
    row_scale = jnp.exp(jax.random.uniform(jax.random.fold_in(key, 22), (SEQ, 1), jnp.float32, jnp.log(0.3), jnp.log(3.0)))
    col_scale = jnp.exp(jax.random.uniform(jax.random.fold_in(key, 23), (1, D), jnp.float32, jnp.log(0.3), jnp.log(3.0)))
    result = base * row_scale * col_scale
    return result.astype(jnp.bfloat16)


def steps_of(stream_key, shape, shards, low, largest):
    level = 1.0
    for dim, parts in shards:
        steps = jax.random.uniform(jax.random.fold_in(jax.random.fold_in(stream_key, 6), dim), (parts,), jnp.float32, low / len(shards), largest / len(shards))
        level = level * jnp.repeat(jnp.exp(steps), shape[dim] // parts).reshape((-1,) + (1,) * (len(shape) - 1 - dim))
    return level


def normal_values(key, extent, scale, most, pieces=(), held_as=jnp.bfloat16):
    values = scale * jax.random.normal(key, extent, jnp.float32)
    if pieces:
        values = values * steps_of(key, extent, pieces, -0.22, 0.18)
    return jnp.clip(values, -most, most).astype(held_as)


def setup_inputs(seed: int = 0) -> dict:
    key_list = jax.random.split(jax.random.key(seed), 12)
    queries = draw_queries(jax.random.fold_in(key_list[11], 71), 0)
    keys = draw_keys(jax.random.fold_in(key_list[11], 71), 0)
    values = draw_values(jax.random.fold_in(key_list[11], 71), 0)
    query_gain = draw_query_gain(jax.random.fold_in(key_list[11], 71), 0)
    key_gain = draw_key_gain(jax.random.fold_in(key_list[11], 71), 0)
    out_weight = normal_values(key_list[5], (HEADS * HEAD_SIZE, D), (HEADS * HEAD_SIZE // 4) ** -0.5, 0.375, ((0, 8),))
    residual = draw_residual(jax.random.fold_in(key_list[11], 71), 0)
    norm_gain = jnp.clip(1.0 + 0.18 * jax.random.normal(key_list[7], (D,), jnp.float32), 0.1, 1.9)
    gate_weight = normal_values(key_list[8], (D, FF), D ** -0.5, 0.125, ((0, 64), (1, 8)))
    up_weight = normal_values(key_list[9], (D, FF), D ** -0.5, 0.125, ((0, 64), (1, 8)))
    down_weight = normal_values(key_list[10], (FF, D), (FF // 4) ** -0.5, 0.15625, ((0, 8), (1, 64)))
    return dict(queries=queries, keys=keys, values=values, query_gain=query_gain, key_gain=key_gain, out_weight=out_weight, residual=residual, norm_gain=norm_gain, gate_weight=gate_weight, up_weight=up_weight, down_weight=down_weight)


epsilon = 1e-06
rope_base = 10000.0

def rotate_pairs(entries, places):
    half = entries.shape[-1] // 2
    frequency = rope_base ** (-jnp.arange(half, dtype=jnp.float32) / half)
    angle = places.astype(jnp.float32)[:, None, None] * frequency[None, None, :]
    cosine = jnp.cos(angle)
    sine = jnp.sin(angle)
    first = entries[..., :half]
    second = entries[..., half:]
    return jnp.concatenate([first * cosine - second * sine, first * sine + second * cosine], axis=-1)

def grid_rotate(entries, grid_rows, grid_cols):
    half = entries.shape[-1] // 2
    return jnp.concatenate([rotate_pairs(entries[..., :half], grid_rows), rotate_pairs(entries[..., half:], grid_cols)], axis=-1)

def head_norm(entries, gains):
    factor = lax.rsqrt(lax.optimization_barrier(jnp.mean(entries * entries, axis=-1, keepdims=True)) + epsilon)
    return entries * factor * gains[None]

def reference(queries, keys, values, query_gain, key_gain, out_weight, residual, norm_gain, gate_weight, up_weight, down_weight):
    length = queries.shape[0]
    heads = query_gain.shape[0]
    key_heads = key_gain.shape[0]
    head_size = query_gain.shape[1]
    group = heads // key_heads
    places = jnp.arange(length, dtype=jnp.int32)
    grid_rows = places // GRID_W
    grid_cols = places % GRID_W
    query_turned = grid_rotate(head_norm(queries.astype(jnp.float32).reshape(length, heads, head_size), query_gain), grid_rows, grid_cols).astype(jnp.bfloat16)
    key_turned = grid_rotate(head_norm(keys.astype(jnp.float32).reshape(length, key_heads, head_size), key_gain), grid_rows, grid_cols).astype(jnp.bfloat16)
    key_wide = key_turned.astype(jnp.float32)
    value_wide = values.reshape(length, key_heads, head_size).astype(jnp.float32)
    scale = head_size ** (-0.5)
    block = math.gcd(length, 128)
    query_blocks = query_turned.reshape(length // block, block, key_heads, group, head_size)

    def attend(query_block):
        scores = jnp.einsum('qgrd,kgd->qgrk', query_block.astype(jnp.float32), key_wide) * scale
        top = lax.optimization_barrier(jnp.max(scores, axis=-1, keepdims=True))
        weights = jnp.exp(scores - top)
        total = lax.optimization_barrier(jnp.sum(weights, axis=-1))
        rounded = lax.optimization_barrier(weights.astype(jnp.bfloat16)).astype(jnp.float32)
        summed = jnp.einsum('qgrk,kgd->qgrd', rounded, value_wide)
        return summed / total[..., None]
    attended = lax.map(attend, query_blocks).reshape(length, heads * head_size).astype(jnp.bfloat16)
    head_cols = heads * head_size // N_TP
    branch = jnp.zeros((length, out_weight.shape[1]), jnp.float32)
    for index in range(N_TP):
        partial_sum = jnp.dot(attended[:, index * head_cols:(index + 1) * head_cols], out_weight[index * head_cols:(index + 1) * head_cols], preferred_element_type=jnp.float32)
        branch = branch + lax.optimization_barrier(partial_sum.astype(jnp.bfloat16)).astype(jnp.float32)
    mid = (residual.astype(jnp.float32) + branch).astype(jnp.bfloat16)
    mid_wide = mid.astype(jnp.float32)
    normed = (mid_wide * lax.rsqrt(lax.optimization_barrier(jnp.mean(mid_wide * mid_wide, axis=-1, keepdims=True)) + epsilon) * norm_gain).astype(jnp.bfloat16)
    gate = jnp.dot(normed, gate_weight, preferred_element_type=jnp.float32)
    up_value = jnp.dot(normed, up_weight, preferred_element_type=jnp.float32)
    hidden = (jax.nn.silu(gate) * up_value).astype(jnp.bfloat16)
    unit_cols = gate_weight.shape[1] // N_TP
    ffn = jnp.zeros((length, down_weight.shape[1]), jnp.float32)
    for index in range(N_TP):
        partial_sum = jnp.dot(hidden[:, index * unit_cols:(index + 1) * unit_cols], down_weight[index * unit_cols:(index + 1) * unit_cols], preferred_element_type=jnp.float32)
        ffn = ffn + lax.optimization_barrier(partial_sum.astype(jnp.bfloat16)).astype(jnp.float32)
    return (mid.astype(jnp.float32) + ffn).astype(jnp.bfloat16)
```

```python
import functools
import jax
import jax.numpy as jnp
from jax import lax
from jax.sharding import PartitionSpec as P
from jax.experimental import pallas as pl
from jax.experimental.pallas import tpu as pltpu

GRID_W = 64
MESH = pl.DeviceIdType.MESH
epsilon = 1e-06
rope_base = 10000.0
Z, Y, X = 16, 4, 4
bf16, f32 = jnp.bfloat16, jnp.float32


def rotate_pairs(entries, places):
    half = entries.shape[-1] // 2
    frequency = rope_base ** (-jnp.arange(half, dtype=f32) / half)
    angle = places.astype(f32)[:, None, None] * frequency[None, None, :]
    cosine = jnp.cos(angle)
    sine = jnp.sin(angle)
    first = entries[..., :half]
    second = entries[..., half:]
    return jnp.concatenate(
        [first * cosine - second * sine, first * sine + second * cosine], axis=-1
    )


def grid_rotate(entries, grid_rows, grid_cols):
    half = entries.shape[-1] // 2
    return jnp.concatenate(
        [
            rotate_pairs(entries[..., :half], grid_rows),
            rotate_pairs(entries[..., half:], grid_cols),
        ],
        axis=-1,
    )


def head_norm(entries, gains):
    factor = lax.rsqrt(jnp.mean(entries * entries, axis=-1, keepdims=True) + epsilon)
    return entries * factor * gains[None]


def nt(a, b):
    return lax.dot_general(a, b, (((1,), (1,)), ((), ())), preferred_element_type=f32)


class Sems:
    def __init__(self):
        self.n = 0

    def __call__(self, count=1):
        at = self.n
        self.n += count
        return at


def plan():
    new = Sems()
    names = {}
    for name, count in (
        ("kvR", 8), ("kvL", 7), ("wR", 8), ("wL", 7), ("wD", 16), ("wy", 2), ("q", 3),
        ("res", 3), ("owx", 3), ("owd", 4), ("comb", 3), ("att", 32),
        ("ra1", 3), ("rb1", 3), ("ra2", 3), ("rb2", 3), ("outx", 3), ("outd", 4),
    ):
        names[name] = (new(count), new(count))
    names["local"] = (new(2), 0)
    return names, new.n


SEMS, NSEMS = plan()


def kernel(
    q_ref, kv_ref, wp_ref, ow_ref, res_ref, ng_ref, out_ref,
    kvb, qb, wb, owb, resb, oacc, macc, cs, cr, ao, att, mid, nrm, hid, part,
    rsa, rsb, a2, b2, rsa2, rsb2, sems,
):
    T = q_ref.shape[0]
    H = T // 2
    HH = H // 2
    D = out_ref.shape[1]
    DX = D // X
    K = kv_ref.shape[1]
    R = wp_ref.shape[2]
    sp = lax.axis_index("sp")
    tp = lax.axis_index("tp")
    z, y, x, c = sp // Y, sp % Y, tp // 2, tp % 2
    o = 1 - c

    def dev(z_, y_, x_, c_):
        return (z_ * Y + y_, x_ * 2 + c_)

    def ss(name, i=0):
        return sems.at[SEMS[name][0] + i]

    def rs(name, i=0):
        return sems.at[SEMS[name][1] + i]

    def remote(src, dst, name, i, to):
        return pltpu.make_async_remote_copy(
            src_ref=src, dst_ref=dst, send_sem=ss(name, i), recv_sem=rs(name, i),
            device_id=to, device_id_type=MESH,
        )

    def got(dst, name, i=0):
        pltpu.make_async_copy(dst, dst, rs(name, i)).wait()

    sent = []

    def go(copy):
        copy.start()
        sent.append(copy)

    barrier = pltpu.get_barrier_semaphore()
    me32 = y * 8 + tp

    def greet(k, _):
        other = lax.rem(me32 + k, 32)
        pl.semaphore_signal(
            barrier, inc=1, device_id=(z * Y + other // 8, other % 8), device_id_type=MESH
        )
        return 0

    lax.fori_loop(1, 32, greet, 0)
    zr, zl = lax.rem(z + 1, Z), lax.rem(z + Z - 1, Z)
    for zz in (zr, zl):
        pl.semaphore_signal(barrier, inc=1, device_id=dev(zz, y, x, c), device_id_type=MESH)
    pl.semaphore_wait(barrier, 33)

    def slot(k):
        return lax.rem(z + k + Z, Z)

    def kv_send(s):
        srcR = kv_ref if s == 0 else kvb.at[slot(-s)]
        go(remote(srcR, kvb.at[slot(-s)], "kvR", s, dev(zr, y, x, c)))
        if s < 7:
            srcL = kv_ref if s == 0 else kvb.at[slot(s)]
            go(remote(srcL, kvb.at[slot(s)], "kvL", s, dev(zl, y, x, c)))

    kv_send(0)
    for k in (1, 2, 3):
        yk = lax.rem(y + k, Y)
        go(remote(q_ref, qb.at[y], "q", k - 1, dev(z, yk, x, c)))
    wrow = pl.ds(pl.multiple_of((z * Y + y) * R, R), R)
    yc = y // 2
    for j in (0, 1):
        to = 2 * c + j
        own = jnp.logical_and(to == y, c == yc)
        src, dst = wp_ref.at[j], wb.at[:, wrow, :]
        far = pltpu.make_async_remote_copy(
            src_ref=src, dst_ref=dst, send_sem=ss("wy", j),
            recv_sem=sems.at[SEMS["wy"][1] + y % 2],
            device_id=dev(z, to, x, yc), device_id_type=MESH,
        )

        @pl.when(jnp.logical_not(own))
        def _():
            far.start()

        @pl.when(own)
        def _():
            pltpu.make_async_copy(src, dst, sems.at[SEMS["wy"][1] + y % 2]).start()

    owrow = pl.ds(pl.multiple_of(tp * 2 * 64, 128), 128)
    for k in (1, 2, 3):
        xk = lax.rem(x + k, X)
        go(remote(ow_ref, owb.at[owrow, :], "owx", k - 1, dev(z, y, xk, c)))
    go(remote(ow_ref, owb.at[owrow, :], "owd", 3, dev(z, y, x, o)))
    own_ow = pltpu.make_async_copy(ow_ref, owb.at[owrow, :], ss("local", 0))
    own_ow.start()
    half = pl.ds(pl.multiple_of(c * H, 32), H)
    own_rows = pl.ds(pl.multiple_of(y * H, 32), H)
    for k in (1, 2, 3):
        yk = lax.rem(y + k, Y)
        go(remote(res_ref.at[half, :], resb.at[own_rows, :], "res", k - 1, dev(z, yk, x, c)))
    own_res = pltpu.make_async_copy(res_ref.at[half, :], resb.at[own_rows, :], ss("local", 1))
    own_res.start()

    def wrows(k, core):
        return wb.at[:, pl.ds(pl.multiple_of((slot(k) * Y + 2 * core) * R, 2 * R), 2 * R), :]

    def w_ring(s):
        if s == 0:
            for i in (0, 1):
                yi = 2 * c + i
                row = pl.ds(pl.multiple_of((z * Y + yi) * R, R), R)
                pltpu.make_async_copy(
                    wb.at[:, row, :], wb.at[:, row, :], sems.at[SEMS["wy"][1] + i]
                ).wait()
        else:
            got(wrows(-s, c), "wR", s - 1)
            if s < 8:
                got(wrows(s, c), "wL", s - 1)
        if s < 8:
            go(remote(wrows(-s, c), wrows(-s, c), "wR", s, dev(zr, y, x, c)))
        if s < 7:
            go(remote(wrows(s, c), wrows(s, c), "wL", s, dev(zl, y, x, c)))
        go(remote(wrows(-s, c), wrows(-s, c), "wD", s, dev(z, y, x, o)))
        if 0 < s < 8:
            go(remote(wrows(s, c), wrows(s, c), "wD", 8 + s, dev(z, y, x, o)))

    def lanes(shape):
        return lax.broadcasted_iota(jnp.int32, shape, 1)

    def attend(blocks, first):
        k0, k1, v0, v1 = [], [], [], []
        for block in blocks:
            kv = block[...].astype(f32)
            turned = pltpu.roll(kv, K // 2, 1)
            low = lanes(kv.shape) < K // 2
            k0.append(jnp.where(low, kv, 0.0).astype(bf16))
            k1.append(jnp.where(low, 0.0, turned).astype(bf16))
            v0.append(jnp.where(low, turned, 1.0).astype(bf16))
            v1.append(jnp.where(low, 1.0, kv).astype(bf16))
        cat = lambda parts: parts[0] if len(parts) == 1 else jnp.concatenate(parts, axis=0)
        keys, vals = (cat(k0), cat(k1)), (cat(v0), cat(v1))

        def rows(j, _):
            q = qb[j]
            for h in (0, 1):
                score = nt(q, keys[h])
                top = jnp.max(score, axis=1, keepdims=True)
                if not first:
                    old = macc[h, j]
                    top = jnp.maximum(old, top)
                    weight = jnp.exp(score - top[:, :1])
                    total = jnp.dot(weight.astype(bf16), vals[h], preferred_element_type=f32)
                    oacc[h, j] = oacc[h, j] * jnp.exp(old - top) + total
                    macc[h, j] = top
                else:
                    weight = jnp.exp(score - top)
                    oacc[h, j] = jnp.dot(
                        weight.astype(bf16), vals[h], preferred_element_type=f32
                    )
                    macc[h, j] = jnp.broadcast_to(top, (T, K))
            return 0

        lax.fori_loop(0, Y, rows, 0)

    qb[y] = q_ref[...]
    for k in (1, 2, 3):
        got(qb.at[lax.rem(y + Y - k, Y)], "q", k - 1)
    w_ring(0)
    attend([kv_ref], True)
    wnext = 1
    for s in range(1, 9):
        got(kvb.at[slot(-s)], "kvR", s - 1)
        if s < 8:
            got(kvb.at[slot(s)], "kvL", s - 1)
            kv_send(s)
        attend([kvb.at[slot(-s)]] + ([kvb.at[slot(s)]] if s < 8 else []), False)
        if s in (2, 3, 4, 5, 6, 7):
            w_ring(wnext)
            wnext += 1

    low = lanes((T, K)) < K // 2
    even = (lanes((T, K)) // (K // 4)) % 2 == 0
    for j in range(Y):
        o0, o1 = oacc[0, j], oacc[1, j]
        total = jnp.where(low, pltpu.roll(o0, K // 2, 1), pltpu.roll(o1, K // 2, 1))
        level = jnp.where(low, macc[0, j], macc[1, j]) + jnp.log(total)
        high = level.astype(bf16)
        rest = (level - high.astype(f32)).astype(bf16)
        cs[j, 0] = (jnp.where(low, o0, o1) / total).astype(bf16)
        cs[j, 1] = jnp.where(even, high.astype(f32), rest.astype(f32)).astype(bf16)
    for k in (1, 2, 3):
        yk = lax.rem(y + k, Y)
        go(remote(cs.at[yk], cr.at[k - 1], "comb", k - 1, dev(z, yk, x, c)))
    w_ring(wnext)
    wnext += 1
    for k in (1, 2, 3):
        got(cr.at[k - 1], "comb", k - 1)

    def level_of(packed):
        wide = packed.astype(f32)
        return wide + jnp.where(
            even, pltpu.roll(wide, K - K // 4, 1), pltpu.roll(wide, K // 4, 1)
        )

    own = cs.at[y]
    outs = [own[0].astype(f32)] + [cr[k, 0].astype(f32) for k in range(3)]
    levels = [level_of(own[1])] + [level_of(cr[k, 1]) for k in range(3)]
    top = functools.reduce(jnp.maximum, levels)
    shares = [jnp.exp(v - top) for v in levels]
    total = sum(shares[1:], shares[0])
    summed = sum((a * b for a, b in zip(outs[1:], shares[1:])), outs[0] * shares[0])
    ao[...] = (summed / total).astype(bf16)

    my_cols = pl.ds(pl.multiple_of(tp * K, K), K)

    def att_copy(k):
        other = lax.rem(me32 + k, 32)
        oc = other % 2
        return remote(
            ao.at[pl.ds(pl.multiple_of(oc * H, 32), H), :], att.at[own_rows, my_cols],
            "att", k, (z * Y + other // 8, other % 8),
        )

    def att_send(k, _):
        att_copy(k).start()
        return 0

    lax.fori_loop(1, 32, att_send, 0)
    att[own_rows, my_cols] = ao[half, :]
    while wnext <= 8:
        w_ring(wnext)
        wnext += 1

    own_ow.wait()
    own_res.wait()
    for k in (1, 2, 3):
        xk = lax.rem(x + X - k, X)
        row = pl.ds(pl.multiple_of((xk * 2 + c) * 128, 128), 128)
        got(owb.at[row, :], "owx", k - 1)
        go(remote(owb.at[row, :], owb.at[row, :], "owd", k - 1, dev(z, y, x, o)))
    for k in (1, 2, 3):
        xk = lax.rem(x + X - k, X)
        got(owb.at[pl.ds(pl.multiple_of((xk * 2 + o) * 128, 128), 128), :], "owd", k - 1)
        yk = lax.rem(y + Y - k, Y)
        got(resb.at[pl.ds(pl.multiple_of(yk * H, 32), H), :], "res", k - 1)
    got(owb.at[pl.ds(pl.multiple_of((x * 2 + o) * 128, 128), 128), :], "owd", 3)

    def att_wait(k, _):
        other = lax.rem(me32 + 32 - k, 32)
        got(
            att.at[
                pl.ds(pl.multiple_of((other // 8) * H, 32), H),
                pl.ds(pl.multiple_of((other % 8) * K, K), K),
            ],
            "att", k,
        )
        return 0

    lax.fori_loop(1, 32, att_wait, 0)

    NB = 512

    def mid_cols(n, square):
        cols = pl.ds(pl.multiple_of(n * NB, NB), NB)
        branch = jnp.dot(att[...], owb[:, cols], preferred_element_type=f32)
        rounded = (resb[:, cols].astype(f32) + branch).astype(bf16)
        mid[:, cols] = rounded
        wide = rounded.astype(f32)
        wide = wide * wide
        return square + sum(wide[:, i * 128 : (i + 1) * 128] for i in range(NB // 128))

    square = lax.fori_loop(0, D // NB, mid_cols, jnp.zeros((Y * H, 128), f32))
    factor = lax.rsqrt(jnp.sum(square, axis=1, keepdims=True) * (1.0 / D) + epsilon)

    def norm_cols(n, _):
        cols = pl.ds(pl.multiple_of(n * NB, NB), NB)
        nrm[:, cols] = (mid[:, cols].astype(f32) * factor * ng_ref[:, cols]).astype(bf16)
        return 0

    lax.fori_loop(0, D // NB, norm_cols, 0)

    for s in range(9):
        got(wrows(-s, o), "wD", s)
        if 0 < s < 8:
            got(wrows(s, o), "wD", 8 + s)
    gate = jnp.dot(nrm[...], wb[0], preferred_element_type=f32)
    up = jnp.dot(nrm[...], wb[1], preferred_element_type=f32)
    hid[...] = (gate / (1.0 + jnp.exp(-gate)) * up).astype(bf16)

    def down_cols(n, _):
        cols = pl.ds(pl.multiple_of(n * NB, NB), NB)
        value = nt(hid[...], wb[2, cols, :]).astype(bf16)
        for j in range(Y):
            part[j, :, cols] = value[j * H : (j + 1) * H]
        return 0

    lax.fori_loop(0, D // NB, down_cols, 0)

    xcols = pl.ds(pl.multiple_of(x * DX, DX), DX)

    def cols_of(xk):
        return pl.ds(pl.multiple_of(xk * DX, DX), DX)

    for k in (1, 2, 3):
        yk = lax.rem(y + k, Y)
        xk = lax.rem(x + k, X)
        go(remote(part.at[yk, pl.ds(0, HH), :], rsa.at[k - 1], "ra1", k - 1, dev(z, yk, x, c)))
        go(
            remote(
                part.at[:, pl.ds(HH, HH), cols_of(xk)], rsb.at[k - 1], "rb1", k - 1,
                dev(z, y, xk, c),
            )
        )
    for k in (1, 2, 3):
        got(rsa.at[k - 1], "ra1", k - 1)
    a2[...] = (
        part[y, :HH, :].astype(f32)
        + rsa[0].astype(f32) + rsa[1].astype(f32) + rsa[2].astype(f32)
    ).astype(bf16)
    for k in (1, 2, 3):
        xk = lax.rem(x + k, X)
        go(remote(a2.at[:, cols_of(xk)], rsa2.at[k - 1], "ra2", k - 1, dev(z, y, xk, c)))
    for k in (1, 2, 3):
        got(rsb.at[k - 1], "rb1", k - 1)
    b2[...] = (
        part[:, HH:, xcols].astype(f32)
        + rsb[0].astype(f32) + rsb[1].astype(f32) + rsb[2].astype(f32)
    ).astype(bf16)
    for k in (1, 2, 3):
        yk = lax.rem(y + k, Y)
        go(remote(b2.at[yk], rsb2.at[k - 1], "rb2", k - 1, dev(z, yk, x, c)))
    for k in (1, 2, 3):
        got(rsa2.at[k - 1], "ra2", k - 1)
    top_rows = pl.ds(pl.multiple_of(c * H, 16), HH)
    low_rows = pl.ds(pl.multiple_of(c * H + HH, 16), HH)
    ffn = (
        a2[:, xcols].astype(f32)
        + rsa2[0].astype(f32) + rsa2[1].astype(f32) + rsa2[2].astype(f32)
    )
    mid_top = mid[pl.ds(pl.multiple_of(y * H, 16), HH), xcols]
    out_ref[top_rows, xcols] = (mid_top.astype(f32) + ffn).astype(bf16)
    for k in (1, 2, 3):
        got(rsb2.at[k - 1], "rb2", k - 1)
    ffn = b2[y].astype(f32) + rsb2[0].astype(f32) + rsb2[1].astype(f32) + rsb2[2].astype(f32)
    mid_low = mid[pl.ds(pl.multiple_of(y * H + HH, 16), HH), xcols]
    out_ref[low_rows, xcols] = (mid_low.astype(f32) + ffn).astype(bf16)

    mine = out_ref.at[half, xcols]
    for k in (1, 2, 3):
        xk = lax.rem(x + k, X)
        go(remote(mine, mine, "outx", k - 1, dev(z, y, xk, c)))
    go(remote(mine, mine, "outd", 3, dev(z, y, x, o)))
    for k in (1, 2, 3):
        piece = out_ref.at[half, cols_of(lax.rem(x + X - k, X))]
        got(piece, "outx", k - 1)
        go(remote(piece, piece, "outd", k - 1, dev(z, y, x, o)))
    other_half = pl.ds(pl.multiple_of(o * H, 32), H)
    for k in (1, 2, 3):
        got(out_ref.at[other_half, cols_of(lax.rem(x + X - k, X))], "outd", k - 1)
    got(out_ref.at[other_half, xcols], "outd", 3)

    for copy in sent:
        copy.wait_send()
    for j in (0, 1):
        to = 2 * c + j

        @pl.when(jnp.logical_not(jnp.logical_and(to == y, c == yc)))
        def _():
            pltpu.make_async_copy(wp_ref.at[j], wp_ref.at[j], ss("wy", j)).wait()

    def att_left(k, _):
        att_copy(k).wait_send()
        return 0

    lax.fori_loop(1, 32, att_left, 0)


def body(
    queries, keys, values, query_gain, key_gain, out_weight, residual, norm_gain,
    gate_weight, up_weight, down_weight,
):
    own = queries.shape[0]
    heads, head_size = query_gain.shape
    key_heads = key_gain.shape[0]
    places = lax.axis_index("sp") * own + jnp.arange(own, dtype=jnp.int32)
    grid_rows = places // GRID_W
    grid_cols = places % GRID_W
    scale = head_size ** (-0.5)
    q = grid_rotate(
        head_norm(queries.astype(f32).reshape(own, heads, head_size), query_gain),
        grid_rows, grid_cols,
    )
    q = (q.astype(bf16) * scale).astype(bf16).reshape(own, heads * head_size)
    k = (
        grid_rotate(
            head_norm(keys.astype(f32).reshape(own, key_heads, head_size), key_gain),
            grid_rows, grid_cols,
        )
        .astype(bf16)
        .reshape(own, key_heads * head_size)
    )
    kv = jnp.concatenate([k, values], axis=1)
    units = gate_weight.shape[1] // 2
    rows = gate_weight.shape[0]
    both = jnp.stack([gate_weight, up_weight, down_weight.T])
    both = both.reshape(3, rows, 2, units)
    padded = -(-units // 128) * 128
    both = jnp.pad(both, ((0, 0), (0, 0), (0, 0), (0, padded - units)))
    pieces = jnp.moveaxis(both, 2, 0)
    D = residual.shape[1]
    T, H, K = own, own // 2, kv.shape[1]
    HH, DX = H // 2, D // X
    vmem = pl.BlockSpec(memory_space=pltpu.VMEM)
    hbm = pl.BlockSpec(memory_space=pl.ANY)
    return pl.pallas_call(
        kernel,
        out_shape=jax.ShapeDtypeStruct((own, D), bf16),
        in_specs=[vmem, vmem, vmem, hbm, hbm, vmem],
        out_specs=vmem,
        scratch_shapes=[
            pltpu.VMEM((Z, T, K), bf16),
            pltpu.VMEM((Y, T, K), bf16),
            pltpu.VMEM((3, D, padded), bf16),
            pltpu.VMEM((8 * K, D), bf16),
            pltpu.VMEM((Y * H, D), bf16),
            pltpu.VMEM((2, Y, T, K), f32),
            pltpu.VMEM((2, Y, T, K), f32),
            pltpu.VMEM((Y, 2, T, K), bf16),
            pltpu.VMEM((3, 2, T, K), bf16),
            pltpu.VMEM((T, K), bf16),
            pltpu.VMEM((Y * H, 8 * K), bf16),
            pltpu.VMEM((Y * H, D), bf16),
            pltpu.VMEM((Y * H, D), bf16),
            pltpu.VMEM((Y * H, padded), bf16),
            pltpu.VMEM((Y, H, D), bf16),
            pltpu.VMEM((3, HH, D), bf16),
            pltpu.VMEM((3, Y, HH, DX), bf16),
            pltpu.VMEM((HH, D), bf16),
            pltpu.VMEM((Y, HH, DX), bf16),
            pltpu.VMEM((3, HH, DX), bf16),
            pltpu.VMEM((3, HH, DX), bf16),
            pltpu.SemaphoreType.DMA((NSEMS,)),
        ],
        compiler_params=pltpu.CompilerParams(
            collective_id=0, has_side_effects=True, vmem_limit_bytes=60 * 1024 * 1024
        ),
    )(q, kv, pieces, out_weight, residual, norm_gain.reshape(1, D))


def solution(mesh):
    in_specs = (
        P("sp", "tp"), P("sp", "tp"), P("sp", "tp"), P("tp", None), P("tp", None),
        P("tp", None), P("sp", None), P(), P("sp", "tp"), P("sp", "tp"), P("tp", "sp"),
    )
    return jax.shard_map(
        body, mesh=mesh, in_specs=in_specs, out_specs=P("sp", None), check_vma=False
    )
```

```python
import functools
import jax
import jax.numpy as jnp
import numpy as np
from jax import lax
from jax.sharding import PartitionSpec as P
from jax.experimental import pallas as pl
from jax.experimental.pallas import tpu as pltpu

GRID_W = 64
MESH = pl.DeviceIdType.MESH
epsilon = 1e-06
rope_base = 10000.0
Z, Y, X = 16, 4, 4
bf16, f32 = jnp.bfloat16, jnp.float32


def rope_tables(count, head_size, width):
    half = head_size // 2
    pairs = half // 2
    lane = np.arange(width) % half
    angle = np.arange(count)[:, None] * rope_base ** (-(lane % pairs) / pairs)[None, :]
    sine = np.where(lane[None, :] < pairs, -np.sin(angle), np.sin(angle))
    return np.stack([np.cos(angle), sine]).astype(np.float32)


def nt(a, b):
    return lax.dot_general(a, b, (((1,), (1,)), ((), ())), preferred_element_type=f32)


class Sems:
    def __init__(self):
        self.n = 0

    def __call__(self, count=1):
        at = self.n
        self.n += count
        return at


def plan():
    new = Sems()
    names = {}
    for name, count in (
        ("kvR", 8), ("kvL", 7), ("wR", 24), ("wL", 21), ("wD", 16), ("wE", 16), ("wy", 2), ("q", 3),
        ("res", 3), ("owx", 3), ("owd", 4), ("comb", 3), ("att", 32),
        ("ra1", 12), ("rb1", 3), ("ra2", 3), ("rb2", 3), ("outx", 3), ("outd", 4),
    ):
        names[name] = (new(count), new(count))
    names["local"] = (new(2), 0)
    names["in"] = (new(10), 0)
    return names, new.n


SEMS, NSEMS = plan()
W_AT = (2, 2, 1, 2)
W_COMB = 3
W_ATT = 9
W_GATE = 0


def kernel(
    q_in, k_in, v_in, qg_in, kg_in, gate_in, up_in, down_in, tab_in,
    ow_ref, res_ref, ng_in, out_ref,
    q_raw, k_raw, v_raw, qg_raw, kg_raw, w_raw, tab, ng_ref,
    q_ref, kv_ref, wp_ref,
    kvb, qb, wb, owb, resb, oacc, macc, cs, cr, ao, att, mid, nrm, hid, part,
    rsa, rsb, a2, b2, rsa2, rsb2, sems,
):
    T = q_ref.shape[0]
    H = T // 2
    HH = H // 2
    D = out_ref.shape[1]
    DX = D // X
    K = kv_ref.shape[1]
    R = wp_ref.shape[2]
    sp = lax.axis_index("sp")
    tp = lax.axis_index("tp")
    z, y, x, c = sp // Y, sp % Y, tp // 2, tp % 2
    o = 1 - c

    def dev(z_, y_, x_, c_):
        return (z_ * Y + y_, x_ * 2 + c_)

    def ss(name, i=0):
        return sems.at[SEMS[name][0] + i]

    def rs(name, i=0):
        return sems.at[SEMS[name][1] + i]

    def remote(src, dst, name, i, to):
        return pltpu.make_async_remote_copy(
            src_ref=src, dst_ref=dst, send_sem=ss(name, i), recv_sem=rs(name, i),
            device_id=to, device_id_type=MESH,
        )

    def got(dst, name, i=0):
        pltpu.make_async_copy(dst, dst, rs(name, i)).wait()

    sent = []

    def go(copy):
        copy.start()
        sent.append(copy)

    ins = [
        pltpu.make_async_copy(src, dst, ss("in", i))
        for i, (src, dst) in enumerate(
            (
                (k_in, k_raw), (v_in, v_raw), (kg_in, kg_raw), (tab_in, tab),
                (q_in, q_raw), (qg_in, qg_raw),
                (gate_in, w_raw.at[0]), (up_in, w_raw.at[1]), (down_in, w_raw.at[2]),
                (ng_in, ng_ref),
            )
        )
    ]
    for copy in ins:
        copy.start()

    barrier = pltpu.get_barrier_semaphore()
    me32 = y * 8 + tp

    def greet(k, _):
        other = lax.rem(me32 + k, 32)
        pl.semaphore_signal(
            barrier, inc=1, device_id=(z * Y + other // 8, other % 8), device_id_type=MESH
        )
        return 0

    lax.fori_loop(1, 32, greet, 0)
    zr, zl = lax.rem(z + 1, Z), lax.rem(z + Z - 1, Z)
    zr2, zl2 = lax.rem(z + 2, Z), lax.rem(z + Z - 2, Z)
    for zz in (zr, zl, zr2, zl2):
        pl.semaphore_signal(barrier, inc=1, device_id=dev(zz, y, x, c), device_id_type=MESH)

    def lanes(shape):
        return lax.broadcasted_iota(jnp.int32, shape, 1)

    S = K // 2
    lane = lanes((T, K))
    rows_in = T // GRID_W

    def table(i):
        by_row = [
            jnp.broadcast_to(tab[i, pl.ds(sp * rows_in + r, 1), :], (GRID_W, K))
            for r in range(rows_in)
        ]
        by_col = jnp.concatenate([tab[i, :GRID_W, :]] * rows_in, axis=0)
        return jnp.where(lane % S < S // 2, jnp.concatenate(by_row, axis=0), by_col)

    def turn(wide, gain):
        square = wide * wide
        low_sum = jnp.sum(jnp.where(lane < S, square, 0.0), axis=1, keepdims=True)
        high_sum = jnp.sum(jnp.where(lane < S, 0.0, square), axis=1, keepdims=True)
        mean = jnp.where(lane < S, low_sum, high_sum) * (1.0 / S)
        normed = wide * lax.rsqrt(mean + epsilon) * gain
        pairs = S // 4
        partner = jnp.where(
            lane % (2 * pairs) < pairs,
            pltpu.roll(normed, K - pairs, 1), pltpu.roll(normed, pairs, 1),
        )
        return (normed * cosine + partner * sine).astype(bf16)

    for copy in ins[:4]:
        copy.wait()
    cosine, sine = table(0), table(1)
    kv = jnp.concatenate([k_raw[...].astype(f32), v_raw[...].astype(f32)], axis=0).T
    key_gain = jnp.concatenate([kg_raw[...], kg_raw[...]], axis=1)
    key_turned = turn(kv, key_gain).astype(f32)
    kv_ref[...] = jnp.where(lane < S, key_turned, kv).astype(bf16)
    pl.semaphore_wait(barrier, 35)

    def slot(k):
        return lax.rem(z + k + Z, Z)

    def kv_send(i):
        left, right = kvb.at[slot(2 * i)], kvb.at[slot(-2 * i)]
        srcL, srcR = (kv_ref, kv_ref) if i == 0 else (left, right)
        go(remote(srcR, right, "kvR", 2 * i + 1, dev(zr2, y, x, c)))
        if i < 3:
            go(remote(srcL, left, "kvL", 2 * i + 1, dev(zl2, y, x, c)))
        go(remote(srcR, right, "kvR", 2 * i, dev(zr, y, x, c)))
        go(remote(srcL, left, "kvL", 2 * i, dev(zl, y, x, c)))

    kv_send(0)
    for copy in ins[4:6]:
        copy.wait()
    query_gain = jnp.concatenate([qg_raw[0:1, :], qg_raw[1:2, :]], axis=1)
    query = turn(q_raw[...].astype(f32), query_gain).astype(f32) * (S ** -0.5)
    q_ref[...] = query.astype(bf16)
    qb[y] = q_ref[...]
    for k in (1, 2, 3):
        yk = lax.rem(y + k, Y)
        go(remote(q_ref, qb.at[y], "q", k - 1, dev(z, yk, x, c)))
    for copy in ins[6:]:
        copy.wait()
    units, padded = w_raw.shape[2] // 2, wp_ref.shape[3]
    wide_lane = lanes((R, padded))
    for m in range(3):
        raw = w_raw[m].astype(f32)
        low_part = jnp.where(wide_lane < units, raw[:, :padded], 0.0)
        high_part = jnp.concatenate(
            [raw[:, units:], jnp.zeros((R, padded - units), f32)], axis=1
        )
        wp_ref[0, m] = low_part.astype(bf16)
        wp_ref[1, m] = high_part.astype(bf16)
    wrow = pl.ds(pl.multiple_of((z * Y + y) * R, R), R)
    yc = y // 2
    for j in (0, 1):
        to = 2 * c + j
        own = jnp.logical_and(to == y, c == yc)
        src, dst = wp_ref.at[j], wb.at[:, wrow, :]
        far = pltpu.make_async_remote_copy(
            src_ref=src, dst_ref=dst, send_sem=ss("wy", j),
            recv_sem=sems.at[SEMS["wy"][1] + y % 2],
            device_id=dev(z, to, x, yc), device_id_type=MESH,
        )

        @pl.when(jnp.logical_not(own))
        def _():
            far.start()

        @pl.when(own)
        def _():
            pltpu.make_async_copy(src, dst, sems.at[SEMS["wy"][1] + y % 2]).start()

    owrow = pl.ds(pl.multiple_of(tp * 2 * 64, 128), 128)
    for k in (1, 2, 3):
        xk = lax.rem(x + k, X)
        go(remote(ow_ref, owb.at[owrow, :], "owx", k - 1, dev(z, y, xk, c)))
    go(remote(ow_ref, owb.at[owrow, :], "owd", 3, dev(z, y, x, o)))
    own_ow = pltpu.make_async_copy(ow_ref, owb.at[owrow, :], ss("local", 0))
    own_ow.start()
    half = pl.ds(pl.multiple_of(c * H, 32), H)
    own_rows = pl.ds(pl.multiple_of(y * H, 32), H)
    own_res = pltpu.make_async_copy(res_ref.at[half, :], resb.at[own_rows, :], ss("local", 1))
    own_res.start()

    def res_send():
        for k in (1, 2, 3):
            yk = lax.rem(y + k, Y)
            go(remote(res_ref.at[half, :], resb.at[own_rows, :], "res", k - 1, dev(z, yk, x, c)))

    res_send()

    def wrows(k, core, m=None):
        rows = pl.ds(pl.multiple_of((slot(k) * Y + 2 * core) * R, 2 * R), 2 * R)
        return wb.at[:, rows, :] if m is None else wb.at[m, rows, :]

    def w_shared(k, core, m):
        rows = pl.ds(pl.multiple_of((slot(k) * Y + 2 * core) * R, 2 * R), 2 * R)
        return wb.at[pl.ds(0, 2) if m == 1 else pl.ds(2, 1), rows, :]

    def w_unit(s, m):
        if s == 0 and m == 0:
            for i in (0, 1):
                yi = 2 * c + i
                row = pl.ds(pl.multiple_of((z * Y + yi) * R, R), R)
                pltpu.make_async_copy(
                    wb.at[:, row, :], wb.at[:, row, :], sems.at[SEMS["wy"][1] + i]
                ).wait()
        if s > 0:
            got(wrows(-s, c, m), "wR", 3 * (s - 1) + m)
        if s < 8:
            block = wrows(-s, c, m)
            go(remote(block, block, "wR", 3 * s + m, dev(zr, y, x, c)))
        if 0 < s < 8:
            got(wrows(s, c, m), "wL", 3 * (s - 1) + m)
        if s < 7:
            block = wrows(s, c, m)
            go(remote(block, block, "wL", 3 * s + m, dev(zl, y, x, c)))
        if m > 0:
            for i, k in ((s, -s), (8 + s, s)):
                if i > 8 and not 0 < s < 8 or i == 8 and s == 0:
                    continue
                share = w_shared(k, c, m)
                go(remote(share, share, "wD" if m == 1 else "wE", i, dev(z, y, x, o)))

    order = [(s + 2 * (m == 2), m, s) for s in range(9) for m in range(3)]
    todo_units = [(s, m) for _, m, s in sorted(order)]

    def w_units(count):
        for unit in todo_units[:count]:
            w_unit(*unit)
        del todo_units[:count]

    def ow_pass(k):
        xk = lax.rem(x + X - k, X)
        row = pl.ds(pl.multiple_of((xk * 2 + c) * 128, 128), 128)
        got(owb.at[row, :], "owx", k - 1)
        go(remote(owb.at[row, :], owb.at[row, :], "owd", k - 1, dev(z, y, x, o)))

    def attend(blocks, first):
        k0, k1, v0, v1 = [], [], [], []
        for block in blocks:
            kv = block[...].astype(f32)
            turned = pltpu.roll(kv, K // 2, 1)
            low = lanes(kv.shape) < K // 2
            k0.append(jnp.where(low, kv, 0.0).astype(bf16))
            k1.append(jnp.where(low, 0.0, turned).astype(bf16))
            v0.append(jnp.where(low, turned, 1.0).astype(bf16))
            v1.append(jnp.where(low, 1.0, kv).astype(bf16))
        cat = lambda parts: parts[0] if len(parts) == 1 else jnp.concatenate(parts, axis=0)
        keys, vals = (cat(k0), cat(k1)), (cat(v0), cat(v1))

        n = keys[0].shape[0]
        todo = [(h, j) for j in range(Y * T // RB) for h in (0, 1)]

        def scores(h, j):
            q = qb[j * RB // T : (j + 1) * RB // T].reshape(RB, K)
            return nt(q, keys[h])

        ahead = scores(*todo[0])
        for i, (h, j) in enumerate(todo):
            score = ahead
            if i + 1 < len(todo):
                ahead = scores(*todo[i + 1])
            rows = pl.ds(j * RB, RB)
            top = jnp.broadcast_to(jnp.max(score, axis=1, keepdims=True), (RB, K))
            if not first:
                old = macc[h, rows]
                top = jnp.maximum(old, top)
            wide = [top] * (n // K) + ([top[:, : n % K]] if n % K else [])
            weight = jnp.exp(score - jnp.concatenate(wide, axis=1))
            total = jnp.dot(weight.astype(bf16), vals[h], preferred_element_type=f32)
            if not first:
                total = oacc[h, rows] * jnp.exp(old - top) + total
            oacc[h, rows] = total
            macc[h, rows] = top

    RB = 2 * T
    for i in range(4):
        near, far = 2 * i + 1, 2 * i + 2
        got(kvb.at[slot(-far)], "kvR", far - 1)
        if i < 3:
            got(kvb.at[slot(far)], "kvL", far - 1)
            kv_send(i + 1)
        got(kvb.at[slot(-near)], "kvR", near - 1)
        got(kvb.at[slot(near)], "kvL", near - 1)
        if i == 0:
            for k in (1, 2, 3):
                got(qb.at[lax.rem(y + Y - k, Y)], "q", k - 1)
        blocks = [kvb.at[slot(k)] for k in ((-near, near, -far, far) if i < 3 else (-near, near, -far))]
        if i == 0:
            attend([kv_ref], True)
        attend(blocks, False)
        w_units(W_AT[i])

    low = lanes((T, K)) < K // 2
    even = (lanes((T, K)) // (K // 4)) % 2 == 0
    for j in range(Y):
        rows = pl.ds(j * T, T)
        o0, o1 = oacc[0, rows], oacc[1, rows]
        total = jnp.where(low, pltpu.roll(o0, K // 2, 1), pltpu.roll(o1, K // 2, 1))
        level = jnp.where(low, macc[0, rows], macc[1, rows]) + jnp.log(total)
        high = level.astype(bf16)
        rest = (level - high.astype(f32)).astype(bf16)
        cs[j, 0] = (jnp.where(low, o0, o1) / total).astype(bf16)
        cs[j, 1] = jnp.where(even, high.astype(f32), rest.astype(f32)).astype(bf16)
    for k in (1, 2, 3):
        yk = lax.rem(y + k, Y)
        go(remote(cs.at[yk], cr.at[k - 1], "comb", k - 1, dev(z, yk, x, c)))
    w_units(W_COMB)
    for k in (1, 2, 3):
        got(cr.at[k - 1], "comb", k - 1)

    def level_of(packed):
        wide = packed.astype(f32)
        return wide + jnp.where(
            even, pltpu.roll(wide, K - K // 4, 1), pltpu.roll(wide, K // 4, 1)
        )

    own = cs.at[y]
    outs = [own[0].astype(f32)] + [cr[k, 0].astype(f32) for k in range(3)]
    levels = [level_of(own[1])] + [level_of(cr[k, 1]) for k in range(3)]
    top = functools.reduce(jnp.maximum, levels)
    shares = [jnp.exp(v - top) for v in levels]
    total = sum(shares[1:], shares[0])
    summed = sum((a * b for a, b in zip(outs[1:], shares[1:])), outs[0] * shares[0])
    ao[...] = (summed / total).astype(bf16)

    my_cols = pl.ds(pl.multiple_of(tp * K, K), K)

    def att_copy(k):
        other = lax.rem(me32 + k, 32)
        oc = other % 2
        return remote(
            ao.at[pl.ds(pl.multiple_of(oc * H, 32), H), :], att.at[own_rows, my_cols],
            "att", k, (z * Y + other // 8, other % 8),
        )

    def att_send(k, _):
        att_copy(k).start()
        return 0

    lax.fori_loop(1, 32, att_send, 0)
    att[own_rows, my_cols] = ao[half, :]
    for k in (1, 2, 3):
        ow_pass(k)
    w_units(W_ATT)

    own_ow.wait()
    own_res.wait()
    for k in (1, 2, 3):
        xk = lax.rem(x + X - k, X)
        got(owb.at[pl.ds(pl.multiple_of((xk * 2 + o) * 128, 128), 128), :], "owd", k - 1)
        yk = lax.rem(y + Y - k, Y)
        got(resb.at[pl.ds(pl.multiple_of(yk * H, 32), H), :], "res", k - 1)
    got(owb.at[pl.ds(pl.multiple_of((x * 2 + o) * 128, 128), 128), :], "owd", 3)

    def att_wait(k, _):
        other = lax.rem(me32 + 32 - k, 32)
        got(
            att.at[
                pl.ds(pl.multiple_of((other // 8) * H, 32), H),
                pl.ds(pl.multiple_of((other % 8) * K, K), K),
            ],
            "att", k,
        )
        return 0

    lax.fori_loop(1, 32, att_wait, 0)

    NB = 512

    def mid_cols(n, square):
        cols = pl.ds(n * NB, NB)
        branch = jnp.dot(att[...], owb[:, cols], preferred_element_type=f32)
        rounded = (resb[:, cols].astype(f32) + branch).astype(bf16)
        mid[:, cols] = rounded
        wide = rounded.astype(f32)
        wide = wide * wide
        return square + sum(wide[:, i * 128 : (i + 1) * 128] for i in range(NB // 128))

    square = jnp.zeros((Y * H, 128), f32)
    for n in range(D // NB):
        square = mid_cols(n, square)
        w_units(1)
    factor = lax.rsqrt(jnp.sum(square, axis=1, keepdims=True) * (1.0 / D) + epsilon)

    def norm_cols(n, _):
        cols = pl.ds(pl.multiple_of(n * NB, NB), NB)
        nrm[:, cols] = (mid[:, cols].astype(f32) * factor * ng_ref[:, cols]).astype(bf16)
        return 0

    lax.fori_loop(0, D // NB, norm_cols, 0)

    w_units(W_GATE)

    def shared_in(m, name):
        for s in range(9):
            got(w_shared(-s, o, m), name, s)
            if 0 < s < 8:
                got(w_shared(s, o, m), name, 8 + s)

    while any(m < 2 for _, m in todo_units):
        w_units(1)
    shared_in(1, "wD")
    gate = jnp.dot(nrm[...], wb[0], preferred_element_type=f32)
    up = jnp.dot(nrm[...], wb[1], preferred_element_type=f32)
    hid[...] = (gate / (1.0 + jnp.exp(-gate)) * up).astype(bf16)

    w_units(len(todo_units))
    shared_in(2, "wE")

    xcols = pl.ds(pl.multiple_of(x * DX, DX), DX)

    def cols_of(xk):
        return pl.ds(pl.multiple_of(xk * DX, DX), DX)

    for k in (1, 2, 3, 4):
        xk = lax.rem(x + k, X)
        cols = cols_of(xk)
        value = nt(hid[...], wb[2, cols, :]).astype(bf16)
        for j in range(Y):
            part[j, :, cols] = value[j * H : (j + 1) * H]
        if k < 4:
            go(
                remote(
                    part.at[:, pl.ds(HH, HH), cols], rsb.at[k - 1], "rb1", k - 1,
                    dev(z, y, xk, c),
                )
            )
        for i in (1, 2, 3):
            yk = lax.rem(y + i, Y)
            go(
                remote(
                    part.at[yk, pl.ds(0, HH), cols], rsa.at[i - 1, :, cols],
                    "ra1", 4 * (i - 1) + k - 1, dev(z, yk, x, c),
                )
            )
    for k in (1, 2, 3):
        for i in range(4):
            got(rsa.at[k - 1, :, cols_of(lax.rem(x + i + 1, X))], "ra1", 4 * (k - 1) + i)
    a2[...] = (
        part[y, :HH, :].astype(f32)
        + rsa[0].astype(f32) + rsa[1].astype(f32) + rsa[2].astype(f32)
    ).astype(bf16)
    for k in (1, 2, 3):
        xk = lax.rem(x + k, X)
        go(remote(a2.at[:, cols_of(xk)], rsa2.at[k - 1], "ra2", k - 1, dev(z, y, xk, c)))
    for k in (1, 2, 3):
        got(rsb.at[k - 1], "rb1", k - 1)
    b2[...] = (
        part[:, HH:, xcols].astype(f32)
        + rsb[0].astype(f32) + rsb[1].astype(f32) + rsb[2].astype(f32)
    ).astype(bf16)
    for k in (1, 2, 3):
        yk = lax.rem(y + k, Y)
        go(remote(b2.at[yk], rsb2.at[k - 1], "rb2", k - 1, dev(z, yk, x, c)))
    for k in (1, 2, 3):
        got(rsa2.at[k - 1], "ra2", k - 1)
    top_rows = pl.ds(pl.multiple_of(c * H, 16), HH)
    low_rows = pl.ds(pl.multiple_of(c * H + HH, 16), HH)
    ffn = (
        a2[:, xcols].astype(f32)
        + rsa2[0].astype(f32) + rsa2[1].astype(f32) + rsa2[2].astype(f32)
    )
    mid_top = mid[pl.ds(pl.multiple_of(y * H, 16), HH), xcols]
    out_ref[top_rows, xcols] = (mid_top.astype(f32) + ffn).astype(bf16)
    for k in (1, 2, 3):
        got(rsb2.at[k - 1], "rb2", k - 1)
    ffn = b2[y].astype(f32) + rsb2[0].astype(f32) + rsb2[1].astype(f32) + rsb2[2].astype(f32)
    mid_low = mid[pl.ds(pl.multiple_of(y * H + HH, 16), HH), xcols]
    out_ref[low_rows, xcols] = (mid_low.astype(f32) + ffn).astype(bf16)

    mine = out_ref.at[half, xcols]
    for k in (1, 2, 3):
        xk = lax.rem(x + k, X)
        go(remote(mine, mine, "outx", k - 1, dev(z, y, xk, c)))
    go(remote(mine, mine, "outd", 3, dev(z, y, x, o)))
    for k in (1, 2, 3):
        piece = out_ref.at[half, cols_of(lax.rem(x + X - k, X))]
        got(piece, "outx", k - 1)
        go(remote(piece, piece, "outd", k - 1, dev(z, y, x, o)))
    other_half = pl.ds(pl.multiple_of(o * H, 32), H)
    for k in (1, 2, 3):
        got(out_ref.at[other_half, cols_of(lax.rem(x + X - k, X))], "outd", k - 1)
    got(out_ref.at[other_half, xcols], "outd", 3)

    for copy in sent:
        copy.wait_send()
    for j in (0, 1):
        to = 2 * c + j

        @pl.when(jnp.logical_not(jnp.logical_and(to == y, c == yc)))
        def _():
            pltpu.make_async_copy(wp_ref.at[j], wp_ref.at[j], ss("wy", j)).wait()

    def att_left(k, _):
        att_copy(k).wait_send()
        return 0

    lax.fori_loop(1, 32, att_left, 0)


def body(
    queries, keys, values, query_gain, key_gain, out_weight, residual, norm_gain,
    gate_weight, up_weight, down_weight,
):
    own = queries.shape[0]
    head_size = query_gain.shape[1]
    K = queries.shape[1]
    tables = jnp.asarray(rope_tables(Z * Y * own // GRID_W, head_size, K))
    rows, width = gate_weight.shape
    padded = -(-(width // 2) // 128) * 128
    D = residual.shape[1]
    T, H = own, own // 2
    HH, DX = H // 2, D // X
    vmem = pl.BlockSpec(memory_space=pltpu.VMEM)
    hbm = pl.BlockSpec(memory_space=pl.ANY)
    return pl.pallas_call(
        kernel,
        out_shape=jax.ShapeDtypeStruct((own, D), bf16),
        in_specs=[hbm] * 12,
        out_specs=vmem,
        scratch_shapes=[
            pltpu.VMEM(queries.shape, bf16),
            pltpu.VMEM(keys.shape[::-1], bf16),
            pltpu.VMEM(values.shape[::-1], bf16),
            pltpu.VMEM(query_gain.shape, f32),
            pltpu.VMEM(key_gain.shape, f32),
            pltpu.VMEM((3, rows, width), bf16),
            pltpu.VMEM(tables.shape, f32),
            pltpu.VMEM((1, D), f32),
            pltpu.VMEM((T, K), bf16),
            pltpu.VMEM((T, K), bf16),
            pltpu.VMEM((2, 3, rows, padded), bf16),
            pltpu.VMEM((Z, T, K), bf16),
            pltpu.VMEM((Y, T, K), bf16),
            pltpu.VMEM((3, D, padded), bf16),
            pltpu.VMEM((8 * K, D), bf16),
            pltpu.VMEM((Y * H, D), bf16),
            pltpu.VMEM((2, Y * T, K), f32),
            pltpu.VMEM((2, Y * T, K), f32),
            pltpu.VMEM((Y, 2, T, K), bf16),
            pltpu.VMEM((3, 2, T, K), bf16),
            pltpu.VMEM((T, K), bf16),
            pltpu.VMEM((Y * H, 8 * K), bf16),
            pltpu.VMEM((Y * H, D), bf16),
            pltpu.VMEM((Y * H, D), bf16),
            pltpu.VMEM((Y * H, padded), bf16),
            pltpu.VMEM((Y, H, D), bf16),
            pltpu.VMEM((3, HH, D), bf16),
            pltpu.VMEM((3, Y, HH, DX), bf16),
            pltpu.VMEM((HH, D), bf16),
            pltpu.VMEM((Y, HH, DX), bf16),
            pltpu.VMEM((3, HH, DX), bf16),
            pltpu.VMEM((3, HH, DX), bf16),
            pltpu.SemaphoreType.DMA((NSEMS,)),
        ],
        compiler_params=pltpu.CompilerParams(
            collective_id=0, has_side_effects=True, vmem_limit_bytes=60 * 1024 * 1024
        ),
    )(
        queries, keys.T, values.T, query_gain, key_gain, gate_weight, up_weight, down_weight.T,
        tables, out_weight, residual, norm_gain.reshape(1, D),
    )


def solution(mesh):
    in_specs = (
        P("sp", "tp"), P("sp", "tp"), P("sp", "tp"), P("tp", None), P("tp", None),
        P("tp", None), P("sp", None), P(), P("sp", "tp"), P("sp", "tp"), P("tp", "sp"),
    )
    return jax.shard_map(
        body, mesh=mesh, in_specs=in_specs, out_specs=P("sp", None), check_vma=False
    )
```

```python
import functools
import jax
import jax.numpy as jnp
import numpy as np
from jax import lax
from jax.sharding import PartitionSpec as P
from jax.experimental import pallas as pl
from jax.experimental.pallas import tpu as pltpu

GRID_W = 64
MESH = pl.DeviceIdType.MESH
epsilon = 1e-06
rope_base = 10000.0
Z, Y, X = 16, 4, 4
bf16, f32 = jnp.bfloat16, jnp.float32


def rope_tables(count, head_size, width):
    half = head_size // 2
    pairs = half // 2
    lane = np.arange(width) % half
    angle = np.arange(count)[:, None] * rope_base ** (-(lane % pairs) / pairs)[None, :]
    sine = np.where(lane[None, :] < pairs, -np.sin(angle), np.sin(angle))
    return np.stack([np.cos(angle), sine]).astype(np.float32)


def nt(a, b):
    return lax.dot_general(a, b, (((1,), (1,)), ((), ())), preferred_element_type=f32)


class Sems:
    def __init__(self):
        self.n = 0

    def __call__(self, count=1):
        at = self.n
        self.n += count
        return at


COPIES = (
    ("kvR", 16), ("kvL", 14), ("wR", 24), ("wL", 21), ("wD", 1), ("wE", 1), ("q", 1),
    ("res", 3), ("resx", 3), ("owx", 3), ("owd", 1), ("comb", 1), ("comt", 1), ("att", 1),
    ("ra1", 4), ("rb1", 4), ("ra2", 1), ("rb2", 1), ("outx", 6), ("outd", 1),
)


def plan():
    new = Sems()
    names = {name: (new(1), new(count)) for name, count in COPIES}
    names["wy"] = (new(2), new(2))
    names["local"] = (new(2), 0)
    names["in"] = (new(10), 0)
    return names, new.n


SEMS, NSEMS = plan()
W_AT = (2, 2, 2, 2)
W_COMB = 4
W_ATT = 9
W_GATE = 0
LAG = 0


def kernel(
    q_in, k_in, v_in, qg_in, kg_in, gate_in, up_in, down_in, tab_in,
    ow_ref, res_ref, ng_in, out_ref,
    q_raw, k_raw, v_raw, qg_raw, kg_raw, w_raw, tab, ng_ref,
    q_ref, kv_ref, wp_ref,
    kvb, qb, wb, owb, resb, oacc, macc, cs, cst, cr, crt, ao, att, mid, nrm, hid, part,
    rsa, rsb, a2, b2, rsa2, rsb2, sems,
):
    T = q_ref.shape[0]
    H = T // 2
    HH = H // 2
    D = out_ref.shape[1]
    DX = D // X
    K = kv_ref.shape[1]
    R = wp_ref.shape[2]
    sp = lax.axis_index("sp")
    tp = lax.axis_index("tp")
    z, y, x, c = sp // Y, sp % Y, tp // 2, tp % 2
    o = 1 - c

    def dev(z_, y_, x_, c_):
        return (z_ * Y + y_, x_ * 2 + c_)

    def ss(name, i=0):
        return sems.at[SEMS[name][0] + i]

    def rs(name, i=0):
        return sems.at[SEMS[name][1] + i]

    def remote(src, dst, name, i, to):
        return pltpu.make_async_remote_copy(
            src_ref=src, dst_ref=dst, send_sem=ss(name), recv_sem=rs(name, i),
            device_id=to, device_id_type=MESH,
        )

    def got(dst, name, i=0):
        pltpu.make_async_copy(dst, dst, rs(name, i)).wait()

    def go(copy):
        copy.start()

    ins = [
        pltpu.make_async_copy(src, dst, ss("in", i))
        for i, (src, dst) in enumerate(
            (
                (k_in, k_raw), (v_in, v_raw), (kg_in, kg_raw), (tab_in, tab),
                (q_in, q_raw), (qg_in, qg_raw),
                (gate_in, w_raw.at[0]), (up_in, w_raw.at[1]), (down_in, w_raw.at[2]),
                (ng_in, ng_ref),
            )
        )
    ]
    for copy in ins:
        copy.start()

    barrier = pltpu.get_barrier_semaphore()
    me32 = y * 8 + tp

    def greet(k, _):
        other = lax.rem(me32 + k, 32)
        pl.semaphore_signal(
            barrier, inc=1, device_id=(z * Y + other // 8, other % 8), device_id_type=MESH
        )
        return 0

    lax.fori_loop(1, 32, greet, 0)
    zr, zl = lax.rem(z + 1, Z), lax.rem(z + Z - 1, Z)
    zr2, zl2 = lax.rem(z + 2, Z), lax.rem(z + Z - 2, Z)
    for zz in (zr, zl, zr2, zl2):
        pl.semaphore_signal(barrier, inc=1, device_id=dev(zz, y, x, c), device_id_type=MESH)

    def lanes(shape):
        return lax.broadcasted_iota(jnp.int32, shape, 1)

    S = K // 2
    lane = lanes((T, K))
    rows_in = T // GRID_W

    def table(i):
        by_row = [
            jnp.broadcast_to(tab[i, pl.ds(sp * rows_in + r, 1), :], (GRID_W, K))
            for r in range(rows_in)
        ]
        by_col = jnp.concatenate([tab[i, :GRID_W, :]] * rows_in, axis=0)
        return jnp.where(lane % S < S // 2, jnp.concatenate(by_row, axis=0), by_col)

    def turn(wide, gain):
        square = wide * wide
        low_sum = jnp.sum(jnp.where(lane < S, square, 0.0), axis=1, keepdims=True)
        high_sum = jnp.sum(jnp.where(lane < S, 0.0, square), axis=1, keepdims=True)
        mean = jnp.where(lane < S, low_sum, high_sum) * (1.0 / S)
        normed = wide * lax.rsqrt(mean + epsilon) * gain
        pairs = S // 4
        partner = jnp.where(
            lane % (2 * pairs) < pairs,
            pltpu.roll(normed, K - pairs, 1), pltpu.roll(normed, pairs, 1),
        )
        return (normed * cosine + partner * sine).astype(bf16)

    for copy in ins[:4]:
        copy.wait()
    cosine, sine = table(0), table(1)
    kv = jnp.concatenate([k_raw[...].astype(f32), v_raw[...].astype(f32)], axis=0).T
    key_gain = jnp.concatenate([kg_raw[...], kg_raw[...]], axis=1)
    key_turned = turn(kv, key_gain).astype(f32)
    kv_ref[...] = jnp.where(lane < S, key_turned, kv).astype(bf16)
    pl.semaphore_wait(barrier, 35)

    def slot(k):
        return lax.rem(z + k + Z, Z)

    def kv_part(k, part_id):
        return kvb.at[slot(k), pl.ds(part_id * H, H), :]

    def kv_far(i, part_id):
        for sign, name, to in ((-1, "kvR", zr2), (1, "kvL", zl2)):
            if sign < 0 or i < 3:
                block = kv_part(sign * 2 * i, part_id)
                src = kv_ref.at[pl.ds(part_id * H, H), :] if i == 0 else block
                go(remote(src, block, name, 2 * (2 * i + 1) + part_id, dev(to, y, x, c)))

    def kv_near(i, part_id):
        for sign, name, to in ((-1, "kvR", zr), (1, "kvL", zl)):
            block = kv_part(sign * 2 * i, part_id)
            src = kv_ref.at[pl.ds(part_id * H, H), :] if i == 0 else block
            go(remote(src, block, name, 2 * (2 * i) + part_id, dev(to, y, x, c)))

    def kv_got(k, part_id):
        got(kv_part(k, part_id), "kvL" if k > 0 else "kvR", 2 * (abs(k) - 1) + part_id)

    for part_id in (0, 1):
        kv_far(0, part_id)
    for part_id in (0, 1):
        kv_near(0, part_id)
    for copy in ins[4:6]:
        copy.wait()
    query_gain = jnp.concatenate([qg_raw[0:1, :], qg_raw[1:2, :]], axis=1)
    query = turn(q_raw[...].astype(f32), query_gain).astype(f32) * (S ** -0.5)
    q_ref[...] = query.astype(bf16)
    qb[y] = q_ref[...]
    for k in (1, 2, 3):
        yk = lax.rem(y + k, Y)
        go(remote(q_ref, qb.at[y], "q", 0, dev(z, yk, x, c)))
    for copy in ins[6:]:
        copy.wait()
    units, padded = w_raw.shape[2] // 2, wp_ref.shape[3]
    wide_lane = lanes((R, padded))
    for m in range(3):
        raw = w_raw[m].astype(f32)
        low_part = jnp.where(wide_lane < units, raw[:, :padded], 0.0)
        high_part = jnp.concatenate(
            [raw[:, units:], jnp.zeros((R, padded - units), f32)], axis=1
        )
        wp_ref[0, m] = low_part.astype(bf16)
        wp_ref[1, m] = high_part.astype(bf16)
    wrow = pl.ds(pl.multiple_of((z * Y + y) * R, R), R)
    yc = y // 2
    for j in (0, 1):
        to = 2 * c + j
        own = jnp.logical_and(to == y, c == yc)
        src, dst = wp_ref.at[j], wb.at[:, wrow, :]
        far = pltpu.make_async_remote_copy(
            src_ref=src, dst_ref=dst, send_sem=ss("wy", j),
            recv_sem=sems.at[SEMS["wy"][1] + y % 2],
            device_id=dev(z, to, x, yc), device_id_type=MESH,
        )

        @pl.when(jnp.logical_not(own))
        def _():
            far.start()

        @pl.when(own)
        def _():
            pltpu.make_async_copy(src, dst, sems.at[SEMS["wy"][1] + y % 2]).start()

    owrow = pl.ds(pl.multiple_of(tp * 2 * 64, 128), 128)
    for k in (1, 2, 3):
        xk = lax.rem(x + k, X)
        go(remote(ow_ref, owb.at[owrow, :], "owx", k - 1, dev(z, y, xk, c)))
    go(remote(ow_ref, owb.at[owrow, :], "owd", 0, dev(z, y, x, o)))
    own_ow = pltpu.make_async_copy(ow_ref, owb.at[owrow, :], ss("local", 0))
    own_ow.start()
    half = pl.ds(pl.multiple_of(c * H, 32), H)
    own_rows = pl.ds(pl.multiple_of(y * H, 32), H)
    own_res = pltpu.make_async_copy(res_ref.at[half, :], resb.at[own_rows, :], ss("local", 1))
    own_res.start()

    y_cols = pl.ds(pl.multiple_of((x % 2) * DX, DX), 3 * DX)
    pass_cols = pl.ds(pl.multiple_of((x % 2) * 3 * DX, DX), DX)
    last_cols = pl.ds(pl.multiple_of((1 - x % 2) * 3 * DX, DX), DX)
    x_pair = x + 1 - 2 * (x % 2)

    def res_rows(k):
        return pl.ds(pl.multiple_of(lax.rem(y + Y - k, Y) * H, 32), H)

    def res_send():
        for k in (1, 2, 3):
            yk = lax.rem(y + k, Y)
            src, dst = res_ref.at[half, y_cols], resb.at[own_rows, y_cols]
            go(remote(src, dst, "res", k - 1, dev(z, yk, x, c)))

    def res_pass():
        for k in (1, 3, 2):
            got(resb.at[res_rows(k), y_cols], "res", k - 1)
            block = resb.at[res_rows(k), pass_cols]
            go(remote(block, block, "resx", k - 1, dev(z, y, x_pair, c)))

    res_send()

    def wrows(k, core, m=None):
        rows = pl.ds(pl.multiple_of((slot(k) * Y + 2 * core) * R, 2 * R), 2 * R)
        return wb.at[:, rows, :] if m is None else wb.at[m, rows, :]

    def w_shared(k, core, m):
        rows = pl.ds(pl.multiple_of((slot(k) * Y + 2 * core) * R, 2 * R), 2 * R)
        return wb.at[pl.ds(0, 2) if m == 1 else pl.ds(2, 1), rows, :]

    def w_unit(s, m):
        if s == 0 and m == 0:
            for i in (0, 1):
                yi = 2 * c + i
                row = pl.ds(pl.multiple_of((z * Y + yi) * R, R), R)
                pltpu.make_async_copy(
                    wb.at[:, row, :], wb.at[:, row, :], sems.at[SEMS["wy"][1] + i]
                ).wait()
        if s > 0:
            got(wrows(-s, c, m), "wR", 3 * (s - 1) + m)
        if s < 8:
            block = wrows(-s, c, m)
            go(remote(block, block, "wR", 3 * s + m, dev(zr, y, x, c)))
        if 0 < s < 8:
            got(wrows(s, c, m), "wL", 3 * (s - 1) + m)
        if s < 7:
            block = wrows(s, c, m)
            go(remote(block, block, "wL", 3 * s + m, dev(zl, y, x, c)))
        if m > 0:
            for i, k in ((s, -s), (8 + s, s)):
                if i > 8 and not 0 < s < 8 or i == 8 and s == 0:
                    continue
                share = w_shared(k, c, m)
                go(remote(share, share, "wD" if m == 1 else "wE", 0, dev(z, y, x, o)))

    order = [(s + LAG * (m == 2), m, s) for s in range(9) for m in range(3)]
    todo_units = [(s, m) for _, m, s in sorted(order)]

    def w_units(count):
        for unit in todo_units[:count]:
            w_unit(*unit)
        del todo_units[:count]

    def ow_pass(k):
        xk = lax.rem(x + X - k, X)
        row = pl.ds(pl.multiple_of((xk * 2 + c) * 128, 128), 128)
        got(owb.at[row, :], "owx", k - 1)
        go(remote(owb.at[row, :], owb.at[row, :], "owd", 0, dev(z, y, x, o)))

    def attend(blocks, first):
        k0, k1, v0, v1 = [], [], [], []
        for block in blocks:
            kv = block[...].astype(f32)
            turned = pltpu.roll(kv, K // 2, 1)
            low = lanes(kv.shape) < K // 2
            k0.append(jnp.where(low, kv, 0.0).astype(bf16))
            k1.append(jnp.where(low, 0.0, turned).astype(bf16))
            v0.append(jnp.where(low, turned, 1.0).astype(bf16))
            v1.append(jnp.where(low, 1.0, kv).astype(bf16))
        cat = lambda parts: parts[0] if len(parts) == 1 else jnp.concatenate(parts, axis=0)
        keys, vals = (cat(k0), cat(k1)), (cat(v0), cat(v1))

        n = keys[0].shape[0]
        todo = [(h, j) for j in range(Y * T // RB) for h in (0, 1)]

        def scores(h, j):
            q = qb[j * RB // T : (j + 1) * RB // T].reshape(RB, K)
            return nt(q, keys[h])

        ahead = scores(*todo[0])
        for i, (h, j) in enumerate(todo):
            score = ahead
            if i + 1 < len(todo):
                ahead = scores(*todo[i + 1])
            rows = pl.ds(j * RB, RB)
            top = jnp.broadcast_to(jnp.max(score, axis=1, keepdims=True), (RB, K))
            if not first:
                old = macc[h, rows]
                top = jnp.maximum(old, top)
            wide = [top] * (n // K) + ([top[:, : n % K]] if n % K else [])
            weight = jnp.exp(score - jnp.concatenate(wide, axis=1))
            total = jnp.dot(weight.astype(bf16), vals[h], preferred_element_type=f32)
            if not first:
                total = oacc[h, rows] * jnp.exp(old - top) + total
            oacc[h, rows] = total
            macc[h, rows] = top

    RB = 2 * T
    got(qb.at[pl.ds(0, 3)], "q")
    attend([kv_ref], True)
    for i in range(4):
        near, far = 2 * i + 1, 2 * i + 2
        for part_id in (0, 1):
            kv_got(-far, part_id)
            if i < 3:
                kv_got(far, part_id)
                kv_far(i + 1, part_id)
        if i < 3:
            for part_id in (0, 1):
                kv_near(i + 1, part_id)
        for part_id in (0, 1):
            kv_got(-near, part_id)
            kv_got(near, part_id)
        blocks = [kvb.at[slot(k)] for k in ((-near, near, -far, far) if i < 3 else (-near, near, -far))]
        attend(blocks, False)
        w_units(W_AT[i])
        if i == 2:
            res_pass()

    low = lanes((T, K)) < K // 2
    for j in range(Y):
        rows = pl.ds(j * T, T)
        o0, o1 = oacc[0, rows], oacc[1, rows]
        total = jnp.where(low, pltpu.roll(o0, K // 2, 1), pltpu.roll(o1, K // 2, 1))
        level = jnp.where(low, macc[0, rows], macc[1, rows]) + jnp.log(total)
        cs[j] = (jnp.where(low, o0, o1) / total).astype(bf16)
        across = level.T
        cst[j, 0:8] = across[0:8]
        cst[j, 8:16] = across[S : S + 8]
    for k in (1, 2, 3):
        yk = lax.rem(y + k, Y)
        go(remote(cst.at[yk], crt.at[k - 1], "comt", 0, dev(z, yk, x, c)))
        go(remote(cs.at[yk], cr.at[k - 1], "comb", 0, dev(z, yk, x, c)))
    w_units(W_COMB)
    got(crt, "comt")
    got(cr, "comb")

    def level_of(across):
        return jnp.concatenate(
            [jnp.broadcast_to(across[i : i + 1], (S, T)) for i in (0, 8)], axis=0
        ).T

    outs = [cs[y].astype(f32)] + [cr[k].astype(f32) for k in range(3)]
    levels = [level_of(cst[y])] + [level_of(crt[k]) for k in range(3)]
    top = functools.reduce(jnp.maximum, levels)
    shares = [jnp.exp(v - top) for v in levels]
    total = sum(shares[1:], shares[0])
    summed = sum((a * b for a, b in zip(outs[1:], shares[1:])), outs[0] * shares[0])
    ao[...] = (summed / total).astype(bf16)

    my_cols = pl.ds(pl.multiple_of(tp * K, K), K)

    def att_copy(k):
        other = lax.rem(me32 + k, 32)
        oc = other % 2
        return remote(
            ao.at[pl.ds(pl.multiple_of(oc * H, 32), H), :], att.at[own_rows, my_cols],
            "att", 0, (z * Y + other // 8, other % 8),
        )

    def att_send(k, _):
        att_copy(k).start()
        return 0

    lax.fori_loop(1, 32, att_send, 0)
    att[own_rows, my_cols] = ao[half, :]
    for k in (1, 2, 3):
        ow_pass(k)
    w_units(W_ATT)

    own_ow.wait()
    own_res.wait()
    for k in (1, 2, 3):
        got(resb.at[res_rows(k), last_cols], "resx", k - 1)
    got(owb.at[pl.ds(0, 4 * 128), :], "owd")

    att_bytes = oacc.at[:, pl.ds(0, 31 * H // 4), :]
    got(att_bytes, "att")

    NB = 512

    def mid_cols(n, square):
        cols = pl.ds(n * NB, NB)
        branch = jnp.dot(att[...], owb[:, cols], preferred_element_type=f32)
        rounded = (resb[:, cols].astype(f32) + branch).astype(bf16)
        mid[:, cols] = rounded
        wide = rounded.astype(f32)
        wide = wide * wide
        return square + sum(wide[:, i * 128 : (i + 1) * 128] for i in range(NB // 128))

    square = jnp.zeros((Y * H, 128), f32)
    for n in range(D // NB):
        square = mid_cols(n, square)
        w_units(1)
    factor = lax.rsqrt(jnp.sum(square, axis=1, keepdims=True) * (1.0 / D) + epsilon)

    def norm_cols(n, _):
        cols = pl.ds(pl.multiple_of(n * NB, NB), NB)
        nrm[:, cols] = (mid[:, cols].astype(f32) * factor * ng_ref[:, cols]).astype(bf16)
        return 0

    lax.fori_loop(0, D // NB, norm_cols, 0)

    w_units(W_GATE)

    shared = {
        "wD": wb.at[pl.ds(0, 2), pl.ds(0, 16 * 2 * R), :],
        "wE": wb.at[pl.ds(2, 1), pl.ds(0, 16 * 2 * R), :],
    }
    while any(m < 2 for _, m in todo_units):
        w_units(1)
    got(shared["wD"], "wD")
    gate = jnp.dot(nrm[...], wb[0], preferred_element_type=f32)
    up = jnp.dot(nrm[...], wb[1], preferred_element_type=f32)
    hid[...] = (gate / (1.0 + jnp.exp(-gate)) * up).astype(bf16)

    w_units(len(todo_units))
    got(shared["wE"], "wE")

    xcols = pl.ds(pl.multiple_of(x * DX, DX), DX)

    def cols_of(xk):
        return pl.ds(pl.multiple_of(xk * DX, DX), DX)

    for k in (1, 2, 3, 4):
        xk = lax.rem(x + k, X)
        cols = cols_of(xk)
        value = nt(hid[...], wb[2, cols, :]).astype(bf16)
        for j in range(Y):
            part[j, :, cols] = value[j * H : (j + 1) * H]
        for i in (1, 2, 3):
            yk = lax.rem(y + i, Y)
            go(
                remote(
                    part.at[yk, pl.ds(0, HH), cols], rsa.at[i - 1, :, cols],
                    "ra1", k - 1, dev(z, yk, x, c),
                )
            )
    for i in (1, 2, 3, 4):
        yk = lax.rem(y + i, Y)
        for k in (1, 2, 3):
            xk = lax.rem(x + k, X)
            go(
                remote(
                    part.at[yk, pl.ds(HH, HH), cols_of(xk)], rsb.at[k - 1, yk],
                    "rb1", i - 1, dev(z, y, xk, c),
                )
            )

    def sum_a(i):
        xk = lax.rem(x + i, X)
        cols = cols_of(xk)
        got(rsa.at[:, :, cols], "ra1", i - 1)
        a2[:, cols] = (
            part[y, :HH, cols].astype(f32) + rsa[0, :, cols].astype(f32)
            + rsa[1, :, cols].astype(f32) + rsa[2, :, cols].astype(f32)
        ).astype(bf16)
        if i < 4:
            go(remote(a2.at[:, cols], rsa2.at[i - 1], "ra2", 0, dev(z, y, xk, c)))

    def sum_b(i):
        yk = lax.rem(y + i, Y)
        got(rsb.at[:, yk], "rb1", i - 1)
        b2[yk] = (
            part[yk, HH:, xcols].astype(f32) + rsb[0, yk].astype(f32)
            + rsb[1, yk].astype(f32) + rsb[2, yk].astype(f32)
        ).astype(bf16)
        if i < 4:
            go(remote(b2.at[yk], rsb2.at[i - 1], "rb2", 0, dev(z, yk, x, c)))

    for i in (1, 2, 3, 4):
        sum_a(i)
        sum_b(i)
    got(rsa2, "ra2")
    top_rows = pl.ds(pl.multiple_of(c * H, 16), HH)
    low_rows = pl.ds(pl.multiple_of(c * H + HH, 16), HH)
    ffn = (
        a2[:, xcols].astype(f32)
        + rsa2[0].astype(f32) + rsa2[1].astype(f32) + rsa2[2].astype(f32)
    )
    mid_top = mid[pl.ds(pl.multiple_of(y * H, 16), HH), xcols]
    out_ref[top_rows, xcols] = (mid_top.astype(f32) + ffn).astype(bf16)

    def out_send(rows, part_id):
        mine = out_ref.at[rows, xcols]
        for k in (1, 2, 3):
            xk = lax.rem(x + k, X)
            go(remote(mine, mine, "outx", 3 * part_id + k - 1, dev(z, y, xk, c)))
        go(remote(mine, mine, "outd", 0, dev(z, y, x, o)))

    def out_pass(rows, part_id):
        for k in (1, 3, 2):
            piece = out_ref.at[rows, cols_of(lax.rem(x + X - k, X))]
            got(piece, "outx", 3 * part_id + k - 1)
            go(remote(piece, piece, "outd", 0, dev(z, y, x, o)))

    out_send(top_rows, 0)
    got(rsb2, "rb2")
    ffn = b2[y].astype(f32) + rsb2[0].astype(f32) + rsb2[1].astype(f32) + rsb2[2].astype(f32)
    mid_low = mid[pl.ds(pl.multiple_of(y * H + HH, 16), HH), xcols]
    out_ref[low_rows, xcols] = (mid_low.astype(f32) + ffn).astype(bf16)
    out_send(low_rows, 1)
    out_pass(top_rows, 0)
    out_pass(low_rows, 1)
    got(rsb.at[pl.ds(0, 2)], "outd")

    def left(ref, name):
        pltpu.make_async_copy(ref, ref, ss(name)).wait()

    left(kvb.at[pl.ds(0, 8)], "kvR")
    left(kvb.at[pl.ds(0, 7)], "kvL")
    left(wb.at[0, pl.ds(0, 24 * 2 * R), :], "wR")
    left(wb.at[0, pl.ds(0, 21 * 2 * R), :], "wL")
    left(shared["wD"], "wD")
    left(shared["wE"], "wE")
    left(qb.at[pl.ds(0, 3)], "q")
    left(resb.at[pl.ds(0, 3 * H), y_cols], "res")
    left(resb.at[pl.ds(0, 3 * H), pass_cols], "resx")
    left(owb.at[pl.ds(0, 3 * 128), :], "owx")
    left(owb.at[pl.ds(0, 4 * 128), :], "owd")
    left(cr, "comb")
    left(crt, "comt")
    left(att_bytes, "att")
    left(rsa, "ra1")
    left(rsb, "rb1")
    left(rsa2, "ra2")
    left(rsb2, "rb2")
    left(rsb.at[pl.ds(0, 2), pl.ds(0, 3)], "outx")
    left(rsb.at[pl.ds(0, 2)], "outd")
    for j in (0, 1):
        to = 2 * c + j

        @pl.when(jnp.logical_not(jnp.logical_and(to == y, c == yc)))
        def _():
            pltpu.make_async_copy(wp_ref.at[j], wp_ref.at[j], ss("wy", j)).wait()


def body(
    queries, keys, values, query_gain, key_gain, out_weight, residual, norm_gain,
    gate_weight, up_weight, down_weight,
):
    own = queries.shape[0]
    head_size = query_gain.shape[1]
    K = queries.shape[1]
    tables = jnp.asarray(rope_tables(Z * Y * own // GRID_W, head_size, K))
    rows, width = gate_weight.shape
    padded = -(-(width // 2) // 128) * 128
    D = residual.shape[1]
    T, H = own, own // 2
    HH, DX = H // 2, D // X
    vmem = pl.BlockSpec(memory_space=pltpu.VMEM)
    hbm = pl.BlockSpec(memory_space=pl.ANY)
    return pl.pallas_call(
        kernel,
        out_shape=pltpu.VMEM((own, D), bf16),
        in_specs=[hbm] * 12,
        out_specs=vmem,
        scratch_shapes=[
            pltpu.VMEM(queries.shape, bf16),
            pltpu.VMEM(keys.shape[::-1], bf16),
            pltpu.VMEM(values.shape[::-1], bf16),
            pltpu.VMEM(query_gain.shape, f32),
            pltpu.VMEM(key_gain.shape, f32),
            pltpu.VMEM((3, rows, width), bf16),
            pltpu.VMEM(tables.shape, f32),
            pltpu.VMEM((1, D), f32),
            pltpu.VMEM((T, K), bf16),
            pltpu.VMEM((T, K), bf16),
            pltpu.VMEM((2, 3, rows, padded), bf16),
            pltpu.VMEM((Z, T, K), bf16),
            pltpu.VMEM((Y, T, K), bf16),
            pltpu.VMEM((3, D, padded), bf16),
            pltpu.VMEM((8 * K, D), bf16),
            pltpu.VMEM((Y * H, D), bf16),
            pltpu.VMEM((2, Y * T, K), f32),
            pltpu.VMEM((2, Y * T, K), f32),
            pltpu.VMEM((Y, T, K), bf16),
            pltpu.VMEM((Y, 16, T), f32),
            pltpu.VMEM((3, T, K), bf16),
            pltpu.VMEM((3, 16, T), f32),
            pltpu.VMEM((T, K), bf16),
            pltpu.VMEM((Y * H, 8 * K), bf16),
            pltpu.VMEM((Y * H, D), bf16),
            pltpu.VMEM((Y * H, D), bf16),
            pltpu.VMEM((Y * H, padded), bf16),
            pltpu.VMEM((Y, H, D), bf16),
            pltpu.VMEM((3, HH, D), bf16),
            pltpu.VMEM((3, Y, HH, DX), bf16),
            pltpu.VMEM((HH, D), bf16),
            pltpu.VMEM((Y, HH, DX), bf16),
            pltpu.VMEM((3, HH, DX), bf16),
            pltpu.VMEM((3, HH, DX), bf16),
            pltpu.SemaphoreType.DMA((NSEMS,)),
        ],
        compiler_params=pltpu.CompilerParams(
            collective_id=0, has_side_effects=True, vmem_limit_bytes=60 * 1024 * 1024
        ),
    )(
        queries, keys.T, values.T, query_gain, key_gain, gate_weight, up_weight, down_weight.T,
        tables, out_weight, residual, norm_gain.reshape(1, D),
    )


def solution(mesh):
    in_specs = (
        P("sp", "tp"), P("sp", "tp"), P("sp", "tp"), P("tp", None), P("tp", None),
        P("tp", None), P("sp", None), P(), P("sp", "tp"), P("sp", "tp"), P("tp", "sp"),
    )
    return jax.shard_map(
        body, mesh=mesh, in_specs=in_specs, out_specs=P("sp", None), check_vma=False
    )
```

```python
import functools
import jax
import jax.numpy as jnp
import numpy as np
from jax import lax
from jax.sharding import PartitionSpec as P
from jax.experimental import pallas as pl
from jax.experimental.pallas import tpu as pltpu

GRID_W = 64
MESH = pl.DeviceIdType.MESH
epsilon = 1e-06
rope_base = 10000.0
Z, Y, X = 16, 4, 4
bf16, f32 = jnp.bfloat16, jnp.float32


def rope_tables(count, head_size, width):
    half = head_size // 2
    pairs = half // 2
    lane = np.arange(width) % half
    angle = np.arange(count)[:, None] * rope_base ** (-(lane % pairs) / pairs)[None, :]
    sine = np.where(lane[None, :] < pairs, -np.sin(angle), np.sin(angle))
    return np.stack([np.cos(angle), sine]).astype(np.float32)


def nt(a, b):
    return lax.dot_general(a, b, (((1,), (1,)), ((), ())), preferred_element_type=f32)


class Sems:
    def __init__(self):
        self.n = 0

    def __call__(self, count=1):
        at = self.n
        self.n += count
        return at


COPIES = (
    ("kvR", 16), ("kvL", 16), ("wR", 24), ("wL", 24), ("wD", 1), ("wE", 1), ("q", 1),
    ("res", 3), ("resx", 3), ("owx", 3), ("owd", 1), ("comb", 1), ("comt", 1), ("att", 1),
    ("ra1", 4), ("rb1", 4), ("ra2", 1), ("rb2", 1), ("outx", 6), ("outd", 1),
)


def plan():
    new = Sems()
    names = {name: (new(1), new(count)) for name, count in COPIES}
    names["wy"] = (new(2), new(2))
    names["local"] = (new(2), 0)
    names["in"] = (new(10), 0)
    return names, new.n


SEMS, NSEMS = plan()
W_FIRST = 0
W_AT = (3, 2, 2, 2)
W_COMB = 4
W_ATT = 9
W_GATE = 0
LAG = 0


def kernel(
    q_in, k_in, v_in, qg_in, kg_in, gate_in, up_in, down_in, tab_in,
    ow_ref, res_ref, ng_in, out_ref,
    q_raw, k_raw, v_raw, qg_raw, kg_raw, w_raw, tab, ng_ref,
    q_ref, kv_ref, wp_ref,
    kvb, qb, wb, owb, resb, oacc, macc, cs, cst, cr, crt, ao, att, mid, nrm, hid, part,
    rsa, rsb, a2, b2, rsa2, rsb2, sems,
):
    T = q_ref.shape[0]
    H = T // 2
    HH = H // 2
    D = out_ref.shape[1]
    DX = D // X
    K = kv_ref.shape[1]
    R = wp_ref.shape[2]
    sp = lax.axis_index("sp")
    tp = lax.axis_index("tp")
    z, y, x, c = sp // Y, sp % Y, tp // 2, tp % 2
    o = 1 - c

    def dev(z_, y_, x_, c_):
        return (z_ * Y + y_, x_ * 2 + c_)

    def ss(name, i=0):
        return sems.at[SEMS[name][0] + i]

    def rs(name, i=0):
        return sems.at[SEMS[name][1] + i]

    def remote(src, dst, name, i, to):
        return pltpu.make_async_remote_copy(
            src_ref=src, dst_ref=dst, send_sem=ss(name), recv_sem=rs(name, i),
            device_id=to, device_id_type=MESH,
        )

    def got(dst, name, i=0):
        pltpu.make_async_copy(dst, dst, rs(name, i)).wait()

    def go(copy):
        copy.start()

    ins = [
        pltpu.make_async_copy(src, dst, ss("in", i))
        for i, (src, dst) in enumerate(
            (
                (k_in, k_raw), (v_in, v_raw), (kg_in, kg_raw), (tab_in, tab),
                (q_in, q_raw), (qg_in, qg_raw),
                (gate_in, w_raw.at[0]), (up_in, w_raw.at[1]), (down_in, w_raw.at[2]),
                (ng_in, ng_ref),
            )
        )
    ]
    for copy in ins:
        copy.start()

    barrier = pltpu.get_barrier_semaphore()
    me32 = y * 8 + tp

    def greet(k, _):
        other = lax.rem(me32 + k, 32)
        pl.semaphore_signal(
            barrier, inc=1, device_id=(z * Y + other // 8, other % 8), device_id_type=MESH
        )
        return 0

    lax.fori_loop(1, 32, greet, 0)
    zr, zl = lax.rem(z + 1, Z), lax.rem(z + Z - 1, Z)
    zr2, zl2 = lax.rem(z + 2, Z), lax.rem(z + Z - 2, Z)
    for zz in (zr, zl, zr2, zl2):
        pl.semaphore_signal(barrier, inc=1, device_id=dev(zz, y, x, c), device_id_type=MESH)

    def lanes(shape):
        return lax.broadcasted_iota(jnp.int32, shape, 1)

    S = K // 2
    lane = lanes((T, K))
    rows_in = T // GRID_W

    def table(i):
        by_row = [
            jnp.broadcast_to(tab[i, pl.ds(sp * rows_in + r, 1), :], (GRID_W, K))
            for r in range(rows_in)
        ]
        by_col = jnp.concatenate([tab[i, :GRID_W, :]] * rows_in, axis=0)
        return jnp.where(lane % S < S // 2, jnp.concatenate(by_row, axis=0), by_col)

    def turn(wide, gain):
        square = wide * wide
        low_sum = jnp.sum(jnp.where(lane < S, square, 0.0), axis=1, keepdims=True)
        high_sum = jnp.sum(jnp.where(lane < S, 0.0, square), axis=1, keepdims=True)
        mean = jnp.where(lane < S, low_sum, high_sum) * (1.0 / S)
        normed = wide * lax.rsqrt(mean + epsilon) * gain
        pairs = S // 4
        partner = jnp.where(
            lane % (2 * pairs) < pairs,
            pltpu.roll(normed, K - pairs, 1), pltpu.roll(normed, pairs, 1),
        )
        return (normed * cosine + partner * sine).astype(bf16)

    for copy in ins[:4]:
        copy.wait()
    cosine, sine = table(0), table(1)
    kv = jnp.concatenate([k_raw[...].astype(f32), v_raw[...].astype(f32)], axis=0).T
    key_gain = jnp.concatenate([kg_raw[...], kg_raw[...]], axis=1)
    key_turned = turn(kv, key_gain).astype(f32)
    kv_ref[...] = jnp.where(lane < S, key_turned, kv).astype(bf16)
    pl.semaphore_wait(barrier, 35)

    def slot(k):
        return lax.rem(z + k + Z, Z)

    def kv_part(k, part_id):
        return kvb.at[slot(k), pl.ds(part_id * H, H), :]

    def kv_far(i, part_id):
        for sign, name, to in ((-1, "kvR", zr2), (1, "kvL", zl2)):
            if i < 3 or part_id == (sign > 0):
                block = kv_part(sign * 2 * i, part_id)
                src = kv_ref.at[pl.ds(part_id * H, H), :] if i == 0 else block
                go(remote(src, block, name, 2 * (2 * i + 1) + part_id, dev(to, y, x, c)))

    def kv_near(i, part_id):
        for sign, name, to in ((-1, "kvR", zr), (1, "kvL", zl)):
            block = kv_part(sign * 2 * i, part_id)
            src = kv_ref.at[pl.ds(part_id * H, H), :] if i == 0 else block
            go(remote(src, block, name, 2 * (2 * i) + part_id, dev(to, y, x, c)))

    def kv_got(k, part_id):
        got(kv_part(k, part_id), "kvL" if k > 0 else "kvR", 2 * (abs(k) - 1) + part_id)

    for part_id in (0, 1):
        kv_far(0, part_id)
    for part_id in (0, 1):
        kv_near(0, part_id)
    for copy in ins[4:6]:
        copy.wait()
    query_gain = jnp.concatenate([qg_raw[0:1, :], qg_raw[1:2, :]], axis=1)
    query = turn(q_raw[...].astype(f32), query_gain).astype(f32) * (S ** -0.5)
    q_ref[...] = query.astype(bf16)
    qb[y] = q_ref[...]
    for k in (1, 2, 3):
        yk = lax.rem(y + k, Y)
        go(remote(q_ref, qb.at[y], "q", 0, dev(z, yk, x, c)))
    for copy in ins[6:]:
        copy.wait()
    units, padded = w_raw.shape[2] // 2, wp_ref.shape[3]
    wide_lane = lanes((R, padded))
    for m in range(3):
        raw = w_raw[m].astype(f32)
        low_part = jnp.where(wide_lane < units, raw[:, :padded], 0.0)
        high_part = jnp.concatenate(
            [raw[:, units:], jnp.zeros((R, padded - units), f32)], axis=1
        )
        wp_ref[0, m] = low_part.astype(bf16)
        wp_ref[1, m] = high_part.astype(bf16)
    wrow = pl.ds(pl.multiple_of((z * Y + y) * R, R), R)
    yc = y // 2
    for j in (0, 1):
        to = 2 * c + j
        own = jnp.logical_and(to == y, c == yc)
        src, dst = wp_ref.at[j], wb.at[:, wrow, :]
        far = pltpu.make_async_remote_copy(
            src_ref=src, dst_ref=dst, send_sem=ss("wy", j),
            recv_sem=sems.at[SEMS["wy"][1] + y % 2],
            device_id=dev(z, to, x, yc), device_id_type=MESH,
        )

        @pl.when(jnp.logical_not(own))
        def _():
            far.start()

        @pl.when(own)
        def _():
            pltpu.make_async_copy(src, dst, sems.at[SEMS["wy"][1] + y % 2]).start()

    owrow = pl.ds(pl.multiple_of(tp * 2 * 64, 128), 128)
    for k in (1, 2, 3):
        xk = lax.rem(x + k, X)
        go(remote(ow_ref, owb.at[owrow, :], "owx", k - 1, dev(z, y, xk, c)))
    go(remote(ow_ref, owb.at[owrow, :], "owd", 0, dev(z, y, x, o)))
    own_ow = pltpu.make_async_copy(ow_ref, owb.at[owrow, :], ss("local", 0))
    own_ow.start()
    half = pl.ds(pl.multiple_of(c * H, 32), H)
    own_rows = pl.ds(pl.multiple_of(y * H, 32), H)
    own_res = pltpu.make_async_copy(res_ref.at[half, :], resb.at[own_rows, :], ss("local", 1))
    own_res.start()

    y_cols = pl.ds(pl.multiple_of((x % 2) * DX, DX), 3 * DX)
    pass_cols = pl.ds(pl.multiple_of((x % 2) * 3 * DX, DX), DX)
    last_cols = pl.ds(pl.multiple_of((1 - x % 2) * 3 * DX, DX), DX)
    x_pair = x + 1 - 2 * (x % 2)

    def res_rows(k):
        return pl.ds(pl.multiple_of(lax.rem(y + Y - k, Y) * H, 32), H)

    def res_send():
        for k in (1, 2, 3):
            yk = lax.rem(y + k, Y)
            src, dst = res_ref.at[half, y_cols], resb.at[own_rows, y_cols]
            go(remote(src, dst, "res", k - 1, dev(z, yk, x, c)))

    def res_pass():
        for k in (1, 3, 2):
            got(resb.at[res_rows(k), y_cols], "res", k - 1)
            block = resb.at[res_rows(k), pass_cols]
            go(remote(block, block, "resx", k - 1, dev(z, y, x_pair, c)))

    def w_block(sign, s, m, one=False):
        one = one or s == 8
        start = (slot(sign * s) * Y + 2 * c) * R + (R if one and sign > 0 else 0)
        size = R if one else 2 * R
        return wb.at[m, pl.ds(pl.multiple_of(start, R), size), :]

    def w_shared(k, core, m):
        rows = pl.ds(pl.multiple_of((slot(k) * Y + 2 * core) * R, 2 * R), 2 * R)
        return wb.at[pl.ds(0, 2) if m == 1 else pl.ds(2, 1), rows, :]

    def w_unit(s, m):
        if s == 0 and m == 0:
            for i in (0, 1):
                yi = 2 * c + i
                row = pl.ds(pl.multiple_of((z * Y + yi) * R, R), R)
                pltpu.make_async_copy(
                    wb.at[:, row, :], wb.at[:, row, :], sems.at[SEMS["wy"][1] + i]
                ).wait()
        for sign, name, to in ((-1, "wR", zr), (1, "wL", zl)):
            if s > 0:
                got(w_block(sign, s, m), name, 3 * (s - 1) + m)
        for sign, name, to in ((-1, "wR", zr), (1, "wL", zl)):
            if s < 8:
                block = w_block(sign, s, m, s == 7)
                go(remote(block, block, name, 3 * s + m, dev(to, y, x, c)))
        if m > 0:
            for i, k in ((s, -s), (8 + s, s)):
                if i > 8 and not 0 < s < 8 or i == 8 and s == 0:
                    continue
                share = w_shared(k, c, m)
                go(remote(share, share, "wD" if m == 1 else "wE", 0, dev(z, y, x, o)))

    order = [(s + LAG * (m == 2), m, s) for s in range(9) for m in range(3)]
    todo_units = [(s, m) for _, m, s in sorted(order)]

    def w_units(count):
        for unit in todo_units[:count]:
            w_unit(*unit)
        del todo_units[:count]

    def ow_pass(k):
        xk = lax.rem(x + X - k, X)
        row = pl.ds(pl.multiple_of((xk * 2 + c) * 128, 128), 128)
        got(owb.at[row, :], "owx", k - 1)
        go(remote(owb.at[row, :], owb.at[row, :], "owd", 0, dev(z, y, x, o)))

    def attend(blocks, first):
        k0, k1, v0, v1 = [], [], [], []
        for block in blocks:
            kv = block[...].astype(f32)
            turned = pltpu.roll(kv, K // 2, 1)
            low = lanes(kv.shape) < K // 2
            k0.append(jnp.where(low, kv, 0.0).astype(bf16))
            k1.append(jnp.where(low, 0.0, turned).astype(bf16))
            v0.append(jnp.where(low, turned, 1.0).astype(bf16))
            v1.append(jnp.where(low, 1.0, kv).astype(bf16))
        cat = lambda parts: parts[0] if len(parts) == 1 else jnp.concatenate(parts, axis=0)
        keys, vals = (cat(k0), cat(k1)), (cat(v0), cat(v1))

        n = keys[0].shape[0]
        todo = [(h, j) for j in range(Y * T // RB) for h in (0, 1)]

        def scores(h, j):
            q = qb[j * RB // T : (j + 1) * RB // T].reshape(RB, K)
            return nt(q, keys[h])

        ahead = scores(*todo[0])
        for i, (h, j) in enumerate(todo):
            score = ahead
            if i + 1 < len(todo):
                ahead = scores(*todo[i + 1])
            rows = pl.ds(j * RB, RB)
            top = jnp.broadcast_to(jnp.max(score, axis=1, keepdims=True), (RB, K))
            if not first:
                old = macc[h, rows]
                top = jnp.maximum(old, top)
            wide = [top] * (n // K) + ([top[:, : n % K]] if n % K else [])
            weight = jnp.exp(score - jnp.concatenate(wide, axis=1))
            total = jnp.dot(weight.astype(bf16), vals[h], preferred_element_type=f32)
            if not first:
                total = oacc[h, rows] * jnp.exp(old - top) + total
            oacc[h, rows] = total
            macc[h, rows] = top

    RB = 2 * T
    got(qb.at[pl.ds(0, 3)], "q")
    res_send()
    attend([kv_ref], True)
    w_units(W_FIRST)
    for i in range(4):
        near, far = 2 * i + 1, 2 * i + 2
        for part_id in (0, 1):
            if i < 3 or part_id == 0:
                kv_got(-far, part_id)
            if i < 3 or part_id == 1:
                kv_got(far, part_id)
            if i < 3:
                kv_far(i + 1, part_id)
        if i < 3:
            for part_id in (0, 1):
                kv_near(i + 1, part_id)
        for part_id in (0, 1):
            kv_got(-near, part_id)
            kv_got(near, part_id)
        blocks = [kvb.at[slot(k)] for k in ((-near, near, -far, far) if i < 3 else (-near, near, -far))]
        attend(blocks, False)
        w_units(W_AT[i])
        if i == 2:
            res_pass()

    low = lanes((T, K)) < K // 2
    for j in range(Y):
        rows = pl.ds(j * T, T)
        o0, o1 = oacc[0, rows], oacc[1, rows]
        total = jnp.where(low, pltpu.roll(o0, K // 2, 1), pltpu.roll(o1, K // 2, 1))
        level = jnp.where(low, macc[0, rows], macc[1, rows]) + jnp.log(total)
        cs[j] = (jnp.where(low, o0, o1) / total).astype(bf16)
        across = level.T
        cst[j, 0:8] = across[0:8]
        cst[j, 8:16] = across[S : S + 8]
    for k in (1, 2, 3):
        yk = lax.rem(y + k, Y)
        go(remote(cst.at[yk], crt.at[k - 1], "comt", 0, dev(z, yk, x, c)))
        go(remote(cs.at[yk], cr.at[k - 1], "comb", 0, dev(z, yk, x, c)))
    w_units(W_COMB)
    got(crt, "comt")
    got(cr, "comb")

    def level_of(across):
        return jnp.concatenate(
            [jnp.broadcast_to(across[i : i + 1], (S, T)) for i in (0, 8)], axis=0
        ).T

    outs = [cs[y].astype(f32)] + [cr[k].astype(f32) for k in range(3)]
    levels = [level_of(cst[y])] + [level_of(crt[k]) for k in range(3)]
    top = functools.reduce(jnp.maximum, levels)
    shares = [jnp.exp(v - top) for v in levels]
    total = sum(shares[1:], shares[0])
    summed = sum((a * b for a, b in zip(outs[1:], shares[1:])), outs[0] * shares[0])
    ao[...] = (summed / total).astype(bf16)

    my_cols = pl.ds(pl.multiple_of(tp * K, K), K)

    def att_copy(k):
        other = lax.rem(me32 + k, 32)
        oc = other % 2
        return remote(
            ao.at[pl.ds(pl.multiple_of(oc * H, 32), H), :], att.at[own_rows, my_cols],
            "att", 0, (z * Y + other // 8, other % 8),
        )

    def att_send(k, _):
        att_copy(k).start()
        return 0

    lax.fori_loop(1, 32, att_send, 0)
    att[own_rows, my_cols] = ao[half, :]
    for k in (1, 2, 3):
        ow_pass(k)
    w_units(W_ATT)

    own_ow.wait()
    own_res.wait()
    for k in (1, 2, 3):
        got(resb.at[res_rows(k), last_cols], "resx", k - 1)
    got(owb.at[pl.ds(0, 4 * 128), :], "owd")

    att_bytes = oacc.at[:, pl.ds(0, 31 * H // 4), :]
    got(att_bytes, "att")

    NB = 512

    def mid_cols(n, square):
        cols = pl.ds(n * NB, NB)
        branch = jnp.dot(att[...], owb[:, cols], preferred_element_type=f32)
        rounded = (resb[:, cols].astype(f32) + branch).astype(bf16)
        mid[:, cols] = rounded
        wide = rounded.astype(f32)
        wide = wide * wide
        return square + sum(wide[:, i * 128 : (i + 1) * 128] for i in range(NB // 128))

    square = jnp.zeros((Y * H, 128), f32)
    for n in range(D // NB):
        square = mid_cols(n, square)
        w_units(1)
    factor = lax.rsqrt(jnp.sum(square, axis=1, keepdims=True) * (1.0 / D) + epsilon)

    def norm_cols(n, _):
        cols = pl.ds(pl.multiple_of(n * NB, NB), NB)
        nrm[:, cols] = (mid[:, cols].astype(f32) * factor * ng_ref[:, cols]).astype(bf16)
        return 0

    lax.fori_loop(0, D // NB, norm_cols, 0)

    w_units(W_GATE)

    shared = {
        "wD": wb.at[pl.ds(0, 2), pl.ds(0, 16 * 2 * R), :],
        "wE": wb.at[pl.ds(2, 1), pl.ds(0, 16 * 2 * R), :],
    }
    while any(m < 2 for _, m in todo_units):
        w_units(1)
    got(shared["wD"], "wD")
    gate = jnp.dot(nrm[...], wb[0], preferred_element_type=f32)
    up = jnp.dot(nrm[...], wb[1], preferred_element_type=f32)
    hid[...] = (gate / (1.0 + jnp.exp(-gate)) * up).astype(bf16)

    w_units(len(todo_units))
    got(shared["wE"], "wE")

    xcols = pl.ds(pl.multiple_of(x * DX, DX), DX)

    def cols_of(xk):
        return pl.ds(pl.multiple_of(xk * DX, DX), DX)

    for k in (1, 2, 3, 4):
        xk = lax.rem(x + k, X)
        cols = cols_of(xk)
        value = nt(hid[...], wb[2, cols, :]).astype(bf16)
        for j in range(Y):
            part[j, :, cols] = value[j * H : (j + 1) * H]
        for i in (1, 2, 3):
            yk = lax.rem(y + i, Y)
            go(
                remote(
                    part.at[yk, pl.ds(0, HH), cols], rsa.at[i - 1, :, cols],
                    "ra1", k - 1, dev(z, yk, x, c),
                )
            )
    for i in (1, 2, 3, 4):
        yk = lax.rem(y + i, Y)
        for k in (1, 2, 3):
            xk = lax.rem(x + k, X)
            go(
                remote(
                    part.at[yk, pl.ds(HH, HH), cols_of(xk)], rsb.at[k - 1, yk],
                    "rb1", i - 1, dev(z, y, xk, c),
                )
            )

    def sum_a(i):
        xk = lax.rem(x + i, X)
        cols = cols_of(xk)
        got(rsa.at[:, :, cols], "ra1", i - 1)
        a2[:, cols] = (
            part[y, :HH, cols].astype(f32) + rsa[0, :, cols].astype(f32)
            + rsa[1, :, cols].astype(f32) + rsa[2, :, cols].astype(f32)
        ).astype(bf16)
        if i < 4:
            go(remote(a2.at[:, cols], rsa2.at[i - 1], "ra2", 0, dev(z, y, xk, c)))

    def sum_b(i):
        yk = lax.rem(y + i, Y)
        got(rsb.at[:, yk], "rb1", i - 1)
        b2[yk] = (
            part[yk, HH:, xcols].astype(f32) + rsb[0, yk].astype(f32)
            + rsb[1, yk].astype(f32) + rsb[2, yk].astype(f32)
        ).astype(bf16)
        if i < 4:
            go(remote(b2.at[yk], rsb2.at[i - 1], "rb2", 0, dev(z, yk, x, c)))

    for i in (1, 2, 3, 4):
        sum_a(i)
        sum_b(i)
    got(rsa2, "ra2")
    top_rows = pl.ds(pl.multiple_of(c * H, 16), HH)
    low_rows = pl.ds(pl.multiple_of(c * H + HH, 16), HH)
    ffn = (
        a2[:, xcols].astype(f32)
        + rsa2[0].astype(f32) + rsa2[1].astype(f32) + rsa2[2].astype(f32)
    )
    mid_top = mid[pl.ds(pl.multiple_of(y * H, 16), HH), xcols]
    out_ref[top_rows, xcols] = (mid_top.astype(f32) + ffn).astype(bf16)

    def out_send(rows, part_id):
        mine = out_ref.at[rows, xcols]
        for k in (1, 2, 3):
            xk = lax.rem(x + k, X)
            go(remote(mine, mine, "outx", 3 * part_id + k - 1, dev(z, y, xk, c)))
        go(remote(mine, mine, "outd", 0, dev(z, y, x, o)))

    def out_pass(rows, part_id):
        for k in (1, 3, 2):
            piece = out_ref.at[rows, cols_of(lax.rem(x + X - k, X))]
            got(piece, "outx", 3 * part_id + k - 1)
            go(remote(piece, piece, "outd", 0, dev(z, y, x, o)))

    out_send(top_rows, 0)
    got(rsb2, "rb2")
    ffn = b2[y].astype(f32) + rsb2[0].astype(f32) + rsb2[1].astype(f32) + rsb2[2].astype(f32)
    mid_low = mid[pl.ds(pl.multiple_of(y * H + HH, 16), HH), xcols]
    out_ref[low_rows, xcols] = (mid_low.astype(f32) + ffn).astype(bf16)
    out_send(low_rows, 1)
    out_pass(top_rows, 0)
    out_pass(low_rows, 1)
    got(rsb.at[pl.ds(0, 2)], "outd")

    def left(ref, name):
        pltpu.make_async_copy(ref, ref, ss(name)).wait()

    for name in ("kvR", "kvL"):
        left(oacc.at[0, pl.ds(0, 15 * H // 2), :], name)
    for name in ("wR", "wL"):
        left(wb.at[0, pl.ds(0, 3 * 15 * R), :], name)
    left(shared["wD"], "wD")
    left(shared["wE"], "wE")
    left(qb.at[pl.ds(0, 3)], "q")
    left(resb.at[pl.ds(0, 3 * H), y_cols], "res")
    left(resb.at[pl.ds(0, 3 * H), pass_cols], "resx")
    left(owb.at[pl.ds(0, 3 * 128), :], "owx")
    left(owb.at[pl.ds(0, 4 * 128), :], "owd")
    left(cr, "comb")
    left(crt, "comt")
    left(att_bytes, "att")
    left(rsa, "ra1")
    left(rsb, "rb1")
    left(rsa2, "ra2")
    left(rsb2, "rb2")
    left(rsb.at[pl.ds(0, 2), pl.ds(0, 3)], "outx")
    left(rsb.at[pl.ds(0, 2)], "outd")
    for j in (0, 1):
        to = 2 * c + j

        @pl.when(jnp.logical_not(jnp.logical_and(to == y, c == yc)))
        def _():
            pltpu.make_async_copy(wp_ref.at[j], wp_ref.at[j], ss("wy", j)).wait()


def body(
    queries, keys, values, query_gain, key_gain, out_weight, residual, norm_gain,
    gate_weight, up_weight, down_weight,
):
    own = queries.shape[0]
    head_size = query_gain.shape[1]
    K = queries.shape[1]
    tables = jnp.asarray(rope_tables(Z * Y * own // GRID_W, head_size, K))
    rows, width = gate_weight.shape
    padded = -(-(width // 2) // 128) * 128
    D = residual.shape[1]
    T, H = own, own // 2
    HH, DX = H // 2, D // X
    vmem = pl.BlockSpec(memory_space=pltpu.VMEM)
    hbm = pl.BlockSpec(memory_space=pl.ANY)
    return pl.pallas_call(
        kernel,
        out_shape=pltpu.VMEM((own, D), bf16),
        in_specs=[hbm] * 12,
        out_specs=vmem,
        scratch_shapes=[
            pltpu.VMEM(queries.shape, bf16),
            pltpu.VMEM(keys.shape[::-1], bf16),
            pltpu.VMEM(values.shape[::-1], bf16),
            pltpu.VMEM(query_gain.shape, f32),
            pltpu.VMEM(key_gain.shape, f32),
            pltpu.VMEM((3, rows, width), bf16),
            pltpu.VMEM(tables.shape, f32),
            pltpu.VMEM((1, D), f32),
            pltpu.VMEM((T, K), bf16),
            pltpu.VMEM((T, K), bf16),
            pltpu.VMEM((2, 3, rows, padded), bf16),
            pltpu.VMEM((Z, T, K), bf16),
            pltpu.VMEM((Y, T, K), bf16),
            pltpu.VMEM((3, D, padded), bf16),
            pltpu.VMEM((8 * K, D), bf16),
            pltpu.VMEM((Y * H, D), bf16),
            pltpu.VMEM((2, Y * T, K), f32),
            pltpu.VMEM((2, Y * T, K), f32),
            pltpu.VMEM((Y, T, K), bf16),
            pltpu.VMEM((Y, 16, T), f32),
            pltpu.VMEM((3, T, K), bf16),
            pltpu.VMEM((3, 16, T), f32),
            pltpu.VMEM((T, K), bf16),
            pltpu.VMEM((Y * H, 8 * K), bf16),
            pltpu.VMEM((Y * H, D), bf16),
            pltpu.VMEM((Y * H, D), bf16),
            pltpu.VMEM((Y * H, padded), bf16),
            pltpu.VMEM((Y, H, D), bf16),
            pltpu.VMEM((3, HH, D), bf16),
            pltpu.VMEM((3, Y, HH, DX), bf16),
            pltpu.VMEM((HH, D), bf16),
            pltpu.VMEM((Y, HH, DX), bf16),
            pltpu.VMEM((3, HH, DX), bf16),
            pltpu.VMEM((3, HH, DX), bf16),
            pltpu.SemaphoreType.DMA((NSEMS,)),
        ],
        compiler_params=pltpu.CompilerParams(
            collective_id=0, has_side_effects=True, vmem_limit_bytes=60 * 1024 * 1024
        ),
    )(
        queries, keys.T, values.T, query_gain, key_gain, gate_weight, up_weight, down_weight.T,
        tables, out_weight, residual, norm_gain.reshape(1, D),
    )


def solution(mesh):
    in_specs = (
        P("sp", "tp"), P("sp", "tp"), P("sp", "tp"), P("tp", None), P("tp", None),
        P("tp", None), P("sp", None), P(), P("sp", "tp"), P("sp", "tp"), P("tp", "sp"),
    )
    return jax.shard_map(
        body, mesh=mesh, in_specs=in_specs, out_specs=P("sp", None), check_vma=False
    )
```
